32 devices in a mesh: ep: 8 (over z, core), tp: 4 (over y, x).
Axes of the slice: x: 2, y: 2, z: 4, core: 2. Of those that a mesh axis runs over, the one named last changes fastest.
Arguments:
- tokens: bfloat16 [1024, 2048], P('ep'), may hold values from -6 to 6
- selected: int32 [8, 256], P(None, 'ep'), may hold values from -1 to 127, as said below
- affinity: float32 [8, 256], P(None, 'ep'), may hold values from 0.05 to 1
- w_gate: bfloat16 [8, 2048, 2048], P('ep', None, 'tp'), may hold values from -0.125 to 0.125
- w_up: bfloat16 [8, 2048, 2048], P('ep', None, 'tp'), may hold values from -0.125 to 0.125
- w_down: bfloat16 [8, 2048, 2048], P('ep', 'tp'), may hold values from -0.125 to 0.125
Outputs:
- combined: bfloat16 [1024, 2048], P('ep', 'tp')
The draws below stay inside these ranges and needn't reach their ends.
Inputs may be any that keep to these rules, and one draw needn't show every extreme that they name: `selected`: row e holds 8 aligned groups of 32 entries; the live entries of group j are distinct positions within the j-th block of 128 tokens, stand at the front of the group and are followed by -1; each row has 128 live entries in all, the number in a group varies, and some group of every row is full.
All inputs are finite; a program needn't handle non-finite values.
Results may differ from the reference program's by a relative error of at most 0.015.
Values may be sent and summed in bfloat16 or wider, within the bound.
A program may use at most 64 MiB of HBM per device.

```python
import math
import jax
import jax.numpy as jnp
from jax import lax

D = 2048
FF = 2048
TOK_DEV = 128
EXPERTS = 8
TOKENS = 1024
PICK = 16
MOST = 32
SLOTS = 256
N_EP = 8
N_TP = 4


def draw_selected(key, part):
    half = N_EP // 2
    block_scores = jax.random.randint(jax.random.fold_in(key, 11), (EXPERTS, N_EP), 0, 2 ** 20)
    block_order = jnp.argsort(block_scores * N_EP + jnp.arange(N_EP, dtype=jnp.int32)[None, :], axis=1, stable=True).astype(jnp.int32)
    inverse = jnp.argsort(block_order, axis=1, stable=True).astype(jnp.int32)
    shifts = jax.random.randint(jax.random.fold_in(key, 12), (EXPERTS, half), -PICK, PICK + 1)
    forced = jax.random.randint(jax.random.fold_in(key, 13), (EXPERTS,), 0, half)
    shifts = jnp.where(jnp.arange(half, dtype=jnp.int32)[None, :] == forced[:, None], PICK, shifts)
    counts_paired = jnp.concatenate([PICK + shifts, PICK - shifts], axis=1)
    counts = jnp.take_along_axis(counts_paired, inverse, axis=1)
    scores = jax.random.randint(jax.random.fold_in(key, 17), (EXPERTS, N_EP, TOK_DEV), 0, 2 ** 20)
    distinct = scores * TOK_DEV + jnp.arange(TOK_DEV, dtype=jnp.int32)[None, None, :]
    order = jnp.argsort(distinct, axis=2, stable=True).astype(jnp.int32)[:, :, :MOST]
    live = jnp.arange(MOST, dtype=jnp.int32)[None, None, :] < counts[:, :, None]
    picked = jnp.where(live, order, -1)
    return picked.reshape(EXPERTS, N_EP * MOST).astype(jnp.int32)


def shard_levels(rng, dims, shards, low, largest):
    loudness = 1.0
    for axis_at, shards_of in shards:
        steps = jax.random.uniform(jax.random.fold_in(jax.random.fold_in(rng, 6), axis_at), (shards_of,), jnp.float32, low / len(shards), largest / len(shards))
        loudness = loudness * jnp.repeat(jnp.exp(steps), dims[axis_at] // shards_of).reshape((-1,) + (1,) * (len(dims) - 1 - axis_at))
    return loudness


def normal_values(stream_key, dims, width, most, pieces=(), kind=jnp.bfloat16):
    values = jax.random.normal(stream_key, dims, jnp.float32) * width
    if len(pieces) > 0:
        values = shard_levels(stream_key, dims, pieces, -0.22, 0.18) * values
    return jnp.clip(values, min=-most, max=most).astype(kind)


def setup_inputs(seed: int = 0) -> dict:
    streams_of = jax.random.split(jax.random.key(seed), 7)
    tokens = normal_values(streams_of[0], (TOKENS, D), 1.0, 6.0, ((0, 8),))
    selected = draw_selected(jax.random.fold_in(streams_of[6], 71), 0)
    affinity = jnp.clip(jnp.exp(math.log(1.0) - 2.9957323 * jax.random.uniform(streams_of[2], (EXPERTS, SLOTS), jnp.float32) ** shard_levels(streams_of[2], (EXPERTS, SLOTS), ((1, 8),), -0.2, 0.2)), 0.05, 1.0)
    w_gate = normal_values(streams_of[3], (EXPERTS, D, FF), D ** -0.5, 0.125, ((0, 8), (2, 4)))
    w_up = normal_values(streams_of[4], (EXPERTS, D, FF), D ** -0.5, 0.125, ((0, 8), (2, 4)))
    w_down = normal_values(streams_of[5], (EXPERTS, FF, D), FF ** -0.5, 0.125, ((0, 8), (1, 4)))
    return {"tokens": tokens, "selected": selected, "affinity": affinity, "w_gate": w_gate, "w_up": w_up, "w_down": w_down}


def reference(tokens, selected, affinity, w_gate, w_up, w_down):
    offsets = (jnp.arange(SLOTS, dtype=jnp.int32) // MOST) * TOK_DEV

    def expert_step(carry, inputs):
        index_row, weight_row, gate_mat, up_mat, down_mat = inputs
        live = index_row >= 0
        position = (jnp.maximum(index_row, 0) + offsets).astype(jnp.int32)
        chosen = tokens[position]
        gate_act = jnp.dot(chosen, gate_mat, preferred_element_type=jnp.float32)
        up_act = jnp.dot(chosen, up_mat, preferred_element_type=jnp.float32)
        hidden = (jax.nn.silu(gate_act) * up_act).astype(jnp.bfloat16)
        blocks = hidden.reshape(SLOTS, N_TP, FF // N_TP).astype(jnp.float32)
        down_blocks = down_mat.reshape(N_TP, FF // N_TP, D).astype(jnp.float32)
        partial_value = jnp.einsum('ckf,kfd->kcd', blocks, down_blocks).astype(jnp.bfloat16)
        expert_out = jnp.sum(partial_value.astype(jnp.float32), axis=0).astype(jnp.bfloat16)
        scaled_weight = jnp.where(live, weight_row, jnp.zeros_like(weight_row))
        carry = carry.at[position].add(scaled_weight[:, None] * expert_out.astype(jnp.float32))
        return carry, None

    initial = jnp.zeros((TOKENS, D), jnp.float32)
    result, unused = lax.scan(expert_step, initial, (selected, affinity, w_gate, w_up, w_down))
    return result.astype(jnp.bfloat16)
```

```python
import functools
import math

import jax
import jax.numpy as jnp
from jax import lax
from jax.experimental import pallas as pl
from jax.experimental.pallas import tpu as pltpu
from jax.sharding import PartitionSpec as P

MESH = pl.DeviceIdType.MESH
F32 = jnp.float32
BF16 = jnp.bfloat16
CHUNK = 128


def side_of(n):
    s = math.isqrt(n)
    while n % s:
        s -= 1
    return s


def plan(n_tp, chunks):
    width = side_of(n_tp)
    height = n_tp // width
    offsets = [(dy, dx) for dy in range(height) for dx in range(width)][1:]
    far = sorted(offsets, key=lambda o: -((o[0] > 0) + (o[1] > 0)))
    extra = list(range(chunks - chunks // 2, chunks)) if (height, width) == (2, 2) else []
    shared = [[o for o in far if not (c in extra and o == (1, 1))] for c in range(chunks)]
    return width, height, far, extra, shared


def kernel(
    n_ep, n_tp, chunks,
    tok_hbm, sel_hbm, aff_hbm, wg_hbm, wu_hbm, wd_hbm, out_ref,
    tok, sel, aff, wgu, wd, onehot, weight_hi, weight_lo, expand, compact,
    cnt_out, cnt_in, z_out, z_in, rows, acc, hid, part_out, part_in, ret_out, ret_in,
    s_in, s_cnt, s_z_r, s_x_r, s_p_r, s_r_r, s_out,
):
    ep = lax.axis_index("ep")
    tp = lax.axis_index("tp")
    n_tok = tok.shape[0]
    n_exp, group = sel.shape
    fc = z_in.shape[2]
    feats = fc * chunks
    live = rows.shape[1]
    hidden = hid.shape[1]
    width, height, far, extra, shared = plan(n_tp, chunks)
    y, x = tp // width, lax.rem(tp, width)

    def tp_to(o):
        return lax.rem(y + o[0], height) * width + lax.rem(x + o[1], width)

    def tp_from(o):
        return lax.rem(y + height - o[0], height) * width + lax.rem(x + width - o[1], width)

    ep_order = list(range(n_ep - 1))
    high_half = ep // (n_ep // 2)

    def ep_to(i):
        down = n_ep - 1 - i
        down = down - jnp.where(down <= ep, 1, 0)
        up = i + jnp.where(i >= ep, 1, 0)
        return jnp.where(high_half > 0, up, down)

    def rows_of(i):
        return pl.ds(pl.multiple_of(i * group, group), group)

    def cols(k, c):
        return pl.ds(pl.multiple_of(k * feats + c * fc, 128), fc)

    def at(c, k):
        return c * n_tp + k

    z_chunks = [(c, (0, 0)) for c in range(chunks)] + [(c, (1, 1)) for c in extra]

    load_sel = pltpu.make_async_copy(sel_hbm, sel, s_in.at[0])
    load_sel.start()
    pltpu.make_async_copy(
        tok_hbm.at[:, pl.ds(pl.multiple_of(tp * feats, 128), feats)],
        tok.at[:, pl.ds(0, feats)], s_in.at[1]).start()
    if extra:
        first = extra[0] * fc
        start = pl.multiple_of(tp_to((1, 1)) * feats + first, 128)
        pltpu.make_async_copy(
            tok_hbm.at[:, pl.ds(start, feats - first)],
            tok.at[:, pl.ds(feats, feats - first)], s_in.at[1]).start()
    load_tok = pltpu.make_async_copy(tok, tok, s_in.at[1])

    barrier = pltpu.get_barrier_semaphore()
    for d in ep_order:
        pl.semaphore_signal(barrier, inc=1, device_id={"ep": ep_to(d)}, device_id_type=MESH)
    for o in far:
        pl.semaphore_signal(barrier, inc=1, device_id={"tp": tp_to(o)}, device_id_type=MESH)

    load_aff = pltpu.make_async_copy(aff_hbm, aff, s_in.at[2])
    load_aff.start()

    load_sel.wait()
    picked = sel[...].astype(F32)
    count = jnp.sum(jnp.where(picked >= 0, 1.0, 0.0), axis=1, keepdims=True)
    for e in range(n_exp):
        cnt_out[e] = jnp.broadcast_to(count[e:e + 1, :], (1, 128))
    picked_t = jnp.transpose(picked)
    token_lane = lax.broadcasted_iota(jnp.int32, (group, n_tok), 1).astype(F32)
    for e in range(n_exp):
        onehot[pl.ds(e * group, group), :] = jnp.where(
            picked_t[:, e:e + 1] == token_lane, 1.0, 0.0)
    load_tok.wait()
    pick = onehot[...].astype(BF16)

    def gather(i):
        z_out[i] = jnp.dot(
            pick, tok[:, i * fc:(i + 1) * fc], preferred_element_type=F32).astype(BF16)
        z_in[i, rows_of(ep), :] = z_out[i, rows_of(ep), :]

    for i in range(len(z_chunks)):
        gather(i)
    cnt_in[ep] = cnt_out[ep]

    pl.semaphore_wait(barrier, len(ep_order) + len(far))

    def send(src, dst, ss, rs, to):
        copy = pltpu.make_async_remote_copy(
            src_ref=src, dst_ref=dst, send_sem=ss, recv_sem=rs,
            device_id=to, device_id_type=MESH)
        copy.start()
        return copy

    others = (n_ep - 1) * group

    def whole(ref, ss, rs):
        return pltpu.make_async_remote_copy(
            src_ref=ref, dst_ref=ref, send_sem=ss, recv_sem=rs,
            device_id={"ep": ep_to(0)}, device_id_type=MESH)

    cnt_all = whole(cnt_in.at[pl.ds(0, n_ep - 1)], s_cnt.at[0], s_cnt.at[1])

    for d in ep_order:
        send(cnt_out.at[ep_to(d)], cnt_in.at[ep], s_cnt.at[0], s_cnt.at[1], {"ep": ep_to(d)})
    for i in range(len(z_chunks)):
        for d in ep_order:
            send(
                z_out.at[i, rows_of(ep_to(d)), :], z_in.at[i, rows_of(ep), :],
                s_out.at[0], s_z_r.at[i], {"ep": ep_to(d)})

    pltpu.make_async_copy(wg_hbm.at[0], wgu.at[:, pl.ds(0, hidden)], s_in.at[3]).start()
    pltpu.make_async_copy(wu_hbm.at[0], wgu.at[:, pl.ds(hidden, hidden)], s_in.at[3]).start()
    load_w = pltpu.make_async_copy(wgu, wgu, s_in.at[3])
    places = far + [(0, 0)]
    for c in range(chunks):
        for n, o in enumerate(places):
            pltpu.make_async_copy(
                wd_hbm.at[0, :, cols(tp_to(o), c)],
                wd.at[c, :, pl.ds(n * fc, fc)], s_in.at[4]).start()
    load_d = pltpu.make_async_copy(wd, wd, s_in.at[4])

    load_aff.wait()
    aff_t = jnp.transpose(aff[...])
    for e in range(n_exp):
        block = pl.ds(e * group, group)
        onehot[block, :] = onehot[block, :] * aff_t[:, e:e + 1]
    weight = jnp.transpose(onehot[...])
    high = weight.astype(BF16)
    weight_hi[...] = high
    weight_lo[...] = (weight - high.astype(F32)).astype(BF16)

    load_w.wait()
    acc[...] = jnp.zeros_like(acc)

    cnt_all.wait_recv()
    lane = lax.broadcasted_iota(jnp.int32, (group, live), 1).astype(F32)
    row = lax.broadcasted_iota(jnp.int32, (group, live), 0).astype(F32)
    begin = jnp.zeros((group, live), F32)
    pieces = []
    for j in range(n_ep):
        n = jnp.broadcast_to(cnt_in[j, 0:1, 0:1], (group, live))
        pieces.append(jnp.where((lane - row == begin) & (row < n), 1.0, 0.0))
        begin = begin + n
    spread = jnp.concatenate(pieces, axis=0)
    expand[...] = spread.astype(BF16)
    compact[...] = jnp.transpose(spread).astype(BF16)

    def take(c, k):
        acc[...] += jnp.dot(rows[at(c, k)], wgu[cols(k, c), :], preferred_element_type=F32)

    def squeeze(i):
        c, o = z_chunks[i]
        whole(z_in.at[i, pl.ds(0, others), :], s_out.at[0], s_z_r.at[i]).wait_recv()
        rows[at(c, tp_to(o))] = jnp.dot(
            compact[...], z_in[i], preferred_element_type=F32).astype(BF16)

    def arrivals(c):
        whole(rows.at[pl.ds(0, len(shared[c]))], s_out.at[1], s_x_r.at[c]).wait_recv()
        for o in shared[c]:
            take(c, tp_from(o))

    for c in range(chunks):
        squeeze(c)
        for o in shared[c]:
            send(
                rows.at[at(c, tp)], rows.at[at(c, tp)],
                s_out.at[1], s_x_r.at[c], {"tp": tp_to(o)})
        take(c, tp)
    for c in range(chunks):
        if c in extra:
            squeeze(chunks + extra.index(c))
            take(c, tp_to((1, 1)))
        arrivals(c)

    gate = acc[:, :hidden]
    up = acc[:, hidden:]
    hid[...] = (gate / (1.0 + jnp.exp(-gate)) * up).astype(BF16)

    load_d.wait()
    step = max(1, 256 // fc)
    for c in range(chunks):
        for n in range(0, n_tp, step):
            some = places[n:n + step]
            value = jnp.dot(
                hid[...], wd[c, :, n * fc:(n + len(some)) * fc], preferred_element_type=F32
            ).astype(BF16)
            for m, o in enumerate(some):
                k = tp_to(o)
                part_out[at(c, k)] = value[:, m * fc:(m + 1) * fc]
                if o != (0, 0):
                    send(
                        part_out.at[at(c, k)], part_in.at[at(c, tp)],
                        s_out.at[2], s_p_r.at[c], {"tp": k})

    for c in range(chunks):
        total = part_out[at(c, tp)].astype(F32)
        whole(part_in.at[pl.ds(0, n_tp - 1)], s_out.at[2], s_p_r.at[c]).wait_recv()
        for o in far:
            total = total + part_in[at(c, tp_from(o))].astype(F32)
        ret_out[c] = jnp.dot(
            expand[...], total.astype(BF16), preferred_element_type=F32).astype(BF16)
        for d in ep_order:
            send(
                ret_out.at[c, rows_of(ep_to(d)), :], ret_in.at[c, rows_of(ep), :],
                s_out.at[3], s_r_r.at[c], {"ep": ep_to(d)})
        ret_in[c, rows_of(ep), :] = ret_out[c, rows_of(ep), :]

    cnt_all.wait_send()
    whole(z_in.at[:, pl.ds(0, others), :], s_out.at[0], s_z_r.at[0]).wait_send()
    n_x = sum(len(s) for s in shared)
    whole(rows.at[pl.ds(0, n_x)], s_out.at[1], s_x_r.at[0]).wait_send()
    whole(part_in.at[pl.ds(0, chunks * (n_tp - 1))], s_out.at[2], s_p_r.at[0]).wait_send()

    for c in range(chunks):
        whole(ret_in.at[c, pl.ds(0, others), :], s_out.at[3], s_r_r.at[c]).wait_recv()
        back = ret_in[c]
        out_ref[:, c * fc:(c + 1) * fc] = (
            jnp.dot(weight_hi[...], back, preferred_element_type=F32)
            + jnp.dot(weight_lo[...], back, preferred_element_type=F32)
        ).astype(BF16)

    whole(ret_in.at[:, pl.ds(0, others), :], s_out.at[3], s_r_r.at[0]).wait_send()


def per_device(tokens, selected, affinity, w_gate, w_up, w_down):
    n_ep = lax.axis_size("ep")
    n_tp = lax.axis_size("tp")
    n_tok, width = tokens.shape
    n_exp, group = selected.shape
    hidden = w_gate.shape[2]
    assert w_gate.shape[0] == 1 and n_exp == n_ep
    feats = width // n_tp
    chunks = max(1, feats // CHUNK)
    fc = feats // chunks
    n_z = chunks + len(plan(n_tp, chunks)[3])
    slots = n_ep * group
    live = slots // 2
    dma = pltpu.SemaphoreType.DMA
    any_spec = pl.BlockSpec(memory_space=pl.ANY)
    return pl.pallas_call(
        functools.partial(kernel, n_ep, n_tp, chunks),
        out_shape=pltpu.VMEM((n_tok, feats), BF16),
        in_specs=[any_spec] * 6,
        out_specs=pl.BlockSpec(memory_space=pltpu.VMEM),
        scratch_shapes=[
            pltpu.VMEM((n_tok, n_z * fc), BF16),
            pltpu.VMEM((n_exp, group), jnp.int32),
            pltpu.VMEM((n_exp, group), F32),
            pltpu.VMEM((width, 2 * hidden), BF16),
            pltpu.VMEM((chunks, hidden, n_tp * fc), BF16),
            pltpu.VMEM((slots, n_tok), F32),
            pltpu.VMEM((n_tok, slots), BF16),
            pltpu.VMEM((n_tok, slots), BF16),
            pltpu.VMEM((slots, live), BF16),
            pltpu.VMEM((live, slots), BF16),
            pltpu.VMEM((n_exp, 1, 128), F32),
            pltpu.VMEM((n_ep, 1, 128), F32),
            pltpu.VMEM((n_z, slots, fc), BF16),
            pltpu.VMEM((n_z, slots, fc), BF16),
            pltpu.VMEM((chunks * n_tp, live, fc), BF16),
            pltpu.VMEM((live, 2 * hidden), F32),
            pltpu.VMEM((live, hidden), BF16),
            pltpu.VMEM((chunks * n_tp, live, fc), BF16),
            pltpu.VMEM((chunks * n_tp, live, fc), BF16),
            pltpu.VMEM((chunks, slots, fc), BF16),
            pltpu.VMEM((chunks, slots, fc), BF16),
            dma((5,)),
            dma((2,)),
            dma((n_z,)),
            dma((chunks,)),
            dma((chunks,)),
            dma((chunks,)),
            dma((4,)),
        ],
        compiler_params=pltpu.CompilerParams(collective_id=0, has_side_effects=True),
    )(tokens, selected, affinity, w_gate, w_up, w_down)


def solution(mesh):
    placed = (
        P("ep", None),
        P(None, "ep"),
        P(None, "ep"),
        P("ep", None, "tp"),
        P("ep", None, "tp"),
        P("ep", "tp", None),
    )
    return jax.shard_map(
        per_device, mesh=mesh, in_specs=placed, out_specs=P("ep", "tp"), check_vma=False
    )
```

```python
import functools
import math

import jax
import jax.numpy as jnp
from jax import lax
from jax.experimental import pallas as pl
from jax.experimental.pallas import tpu as pltpu
from jax.sharding import PartitionSpec as P

MESH = pl.DeviceIdType.MESH
F32 = jnp.float32
BF16 = jnp.bfloat16
CHUNK = 128
EXTRA = 2
LATE = {1: [4], 2: [5]}


def side_of(n):
    s = math.isqrt(n)
    while n % s:
        s -= 1
    return s


def plan(n_tp, chunks):
    width = side_of(n_tp)
    height = n_tp // width
    offsets = [(dy, dx) for dy in range(height) for dx in range(width)][1:]
    far = sorted(offsets, key=lambda o: -((o[0] > 0) + (o[1] > 0)))
    extra = list(range(chunks - EXTRA, chunks)) if (height, width) == (2, 2) else []
    shared = [[o for o in far if not (c in extra and o == (1, 1))] for c in range(chunks)]
    return width, height, far, extra, shared


def kernel(
    n_ep, n_tp, chunks,
    tok_hbm, sel_hbm, aff_hbm, wg_hbm, wu_hbm, wd_hbm, out_ref,
    tok, sel, aff, wgu, wd, onehot, weight_hi, weight_lo, expand, compact,
    cnt_out, cnt_in, z_out, z_in, rows, acc, hid, part_out, part_in, ret_out, ret_in,
    s_in, s_cnt, s_z_r, s_x_r, s_p_r, s_r_r, s_out,
):
    ep = lax.axis_index("ep")
    tp = lax.axis_index("tp")
    n_tok = tok.shape[0]
    n_exp, group = sel.shape
    fc = z_in.shape[2]
    feats = fc * chunks
    live = rows.shape[1]
    hidden = hid.shape[1]
    width, height, far, extra, shared = plan(n_tp, chunks)
    y, x = tp // width, lax.rem(tp, width)

    def tp_to(o):
        return lax.rem(y + o[0], height) * width + lax.rem(x + o[1], width)

    def tp_from(o):
        return lax.rem(y + height - o[0], height) * width + lax.rem(x + width - o[1], width)

    ep_order = list(range(n_ep - 1))
    high_half = ep // (n_ep // 2)

    def ep_to(i):
        down = n_ep - 1 - i
        down = down - jnp.where(down <= ep, 1, 0)
        up = i + jnp.where(i >= ep, 1, 0)
        return jnp.where(high_half > 0, up, down)

    def rows_of(i):
        return pl.ds(pl.multiple_of(i * group, group), group)

    def cols(k, c):
        return pl.ds(pl.multiple_of(k * feats + c * fc, 128), fc)

    def at(c, k):
        return c * n_tp + k

    z_chunks = [(c, (0, 0)) for c in range(chunks)] + [(c, (1, 1)) for c in extra]

    load_sel = pltpu.make_async_copy(sel_hbm, sel, s_in.at[0])
    load_sel.start()
    pltpu.make_async_copy(
        tok_hbm.at[:, pl.ds(pl.multiple_of(tp * feats, 128), feats)],
        tok.at[:, pl.ds(0, feats)], s_in.at[1]).start()
    if extra:
        first = extra[0] * fc
        start = pl.multiple_of(tp_to((1, 1)) * feats + first, 128)
        pltpu.make_async_copy(
            tok_hbm.at[:, pl.ds(start, feats - first)],
            tok.at[:, pl.ds(feats, feats - first)], s_in.at[1]).start()
    load_tok = pltpu.make_async_copy(tok, tok, s_in.at[1])

    barrier = pltpu.get_barrier_semaphore()
    for d in ep_order:
        pl.semaphore_signal(barrier, inc=1, device_id={"ep": ep_to(d)}, device_id_type=MESH)
    for o in far:
        pl.semaphore_signal(barrier, inc=1, device_id={"tp": tp_to(o)}, device_id_type=MESH)

    load_aff = pltpu.make_async_copy(aff_hbm, aff, s_in.at[2])
    load_aff.start()

    load_sel.wait()
    picked = sel[...].astype(F32)
    count = jnp.sum(jnp.where(picked >= 0, 1.0, 0.0), axis=1, keepdims=True)
    for e in range(n_exp):
        cnt_out[e] = jnp.broadcast_to(count[e:e + 1, :], (1, 128))
    picked_t = jnp.transpose(picked)
    token_lane = lax.broadcasted_iota(jnp.int32, (group, n_tok), 1).astype(F32)
    for e in range(n_exp):
        onehot[pl.ds(e * group, group), :] = jnp.where(
            picked_t[:, e:e + 1] == token_lane, 1.0, 0.0)
    load_tok.wait()
    pick = onehot[...].astype(BF16)

    def gather(i):
        z_out[i] = jnp.dot(
            pick, tok[:, i * fc:(i + 1) * fc], preferred_element_type=F32).astype(BF16)
        z_in[i, rows_of(ep), :] = z_out[i, rows_of(ep), :]

    for i in range(len(z_chunks)):
        gather(i)
    cnt_in[ep] = cnt_out[ep]

    pl.semaphore_wait(barrier, len(ep_order) + len(far))

    def send(src, dst, ss, rs, to):
        copy = pltpu.make_async_remote_copy(
            src_ref=src, dst_ref=dst, send_sem=ss, recv_sem=rs,
            device_id=to, device_id_type=MESH)
        copy.start()
        return copy

    others = (n_ep - 1) * group

    def whole(ref, ss, rs):
        return pltpu.make_async_remote_copy(
            src_ref=ref, dst_ref=ref, send_sem=ss, recv_sem=rs,
            device_id={"ep": ep_to(0)}, device_id_type=MESH)

    cnt_all = whole(cnt_in.at[pl.ds(0, n_ep - 1)], s_cnt.at[0], s_cnt.at[1])

    for d in ep_order:
        send(cnt_out.at[ep_to(d)], cnt_in.at[ep], s_cnt.at[0], s_cnt.at[1], {"ep": ep_to(d)})
    def spread_out(i):
        for d in ep_order:
            send(
                z_out.at[i, rows_of(ep_to(d)), :], z_in.at[i, rows_of(ep), :],
                s_out.at[0], s_z_r.at[i], {"ep": ep_to(d)})

    for i in range(chunks):
        spread_out(i)

    pltpu.make_async_copy(wg_hbm.at[0], wgu.at[:, pl.ds(0, hidden)], s_in.at[3]).start()
    pltpu.make_async_copy(wu_hbm.at[0], wgu.at[:, pl.ds(hidden, hidden)], s_in.at[3]).start()
    load_w = pltpu.make_async_copy(wgu, wgu, s_in.at[3])
    places = far + [(0, 0)]
    for c in range(chunks):
        for n, o in enumerate(places):
            pltpu.make_async_copy(
                wd_hbm.at[0, :, cols(tp_to(o), c)],
                wd.at[c, :, pl.ds(n * fc, fc)], s_in.at[4]).start()
    load_d = pltpu.make_async_copy(wd, wd, s_in.at[4])

    load_aff.wait()
    aff_t = jnp.transpose(aff[...])
    for e in range(n_exp):
        block = pl.ds(e * group, group)
        onehot[block, :] = onehot[block, :] * aff_t[:, e:e + 1]
    weight = jnp.transpose(onehot[...])
    high = weight.astype(BF16)
    weight_hi[...] = high
    weight_lo[...] = (weight - high.astype(F32)).astype(BF16)

    load_w.wait()
    acc[...] = jnp.zeros_like(acc)

    cnt_all.wait_recv()
    lane = lax.broadcasted_iota(jnp.int32, (group, live), 1).astype(F32)
    row = lax.broadcasted_iota(jnp.int32, (group, live), 0).astype(F32)
    begin = jnp.zeros((group, live), F32)
    pieces = []
    for j in range(n_ep):
        n = jnp.broadcast_to(cnt_in[j, 0:1, 0:1], (group, live))
        pieces.append(jnp.where((lane - row == begin) & (row < n), 1.0, 0.0))
        begin = begin + n
    spread = jnp.concatenate(pieces, axis=0)
    expand[...] = spread.astype(BF16)
    compact[...] = jnp.transpose(spread).astype(BF16)

    def take(c, k):
        acc[...] += jnp.dot(rows[at(c, k)], wgu[cols(k, c), :], preferred_element_type=F32)

    def squeeze(i):
        c, o = z_chunks[i]
        whole(z_in.at[i, pl.ds(0, others), :], s_out.at[0], s_z_r.at[i]).wait_recv()
        rows[at(c, tp_to(o))] = jnp.dot(
            compact[...], z_in[i], preferred_element_type=F32).astype(BF16)

    def arrivals(c):
        whole(rows.at[pl.ds(0, len(shared[c]))], s_out.at[1], s_x_r.at[c]).wait_recv()
        for o in shared[c]:
            take(c, tp_from(o))

    for c in range(chunks):
        squeeze(c)
        for o in shared[c]:
            send(
                rows.at[at(c, tp)], rows.at[at(c, tp)],
                s_out.at[1], s_x_r.at[c], {"tp": tp_to(o)})
        for i in LATE.get(c, ()):
            if i < len(z_chunks):
                spread_out(i)
        take(c, tp)
    for c in range(chunks):
        if c in extra:
            squeeze(chunks + extra.index(c))
            take(c, tp_to((1, 1)))
        arrivals(c)

    gate = acc[:, :hidden]
    up = acc[:, hidden:]
    hid[...] = (gate / (1.0 + jnp.exp(-gate)) * up).astype(BF16)

    load_d.wait()
    step = max(1, 256 // fc)
    for c in range(chunks):
        for n in range(0, n_tp, step):
            some = places[n:n + step]
            value = jnp.dot(
                hid[...], wd[c, :, n * fc:(n + len(some)) * fc], preferred_element_type=F32
            ).astype(BF16)
            for m, o in enumerate(some):
                k = tp_to(o)
                part_out[at(c, k)] = value[:, m * fc:(m + 1) * fc]
                if o != (0, 0):
                    send(
                        part_out.at[at(c, k)], part_in.at[at(c, tp)],
                        s_out.at[2], s_p_r.at[c], {"tp": k})

    for c in range(chunks):
        total = part_out[at(c, tp)].astype(F32)
        whole(part_in.at[pl.ds(0, n_tp - 1)], s_out.at[2], s_p_r.at[c]).wait_recv()
        for o in far:
            total = total + part_in[at(c, tp_from(o))].astype(F32)
        ret_out[c] = jnp.dot(
            expand[...], total.astype(BF16), preferred_element_type=F32).astype(BF16)
        for d in ep_order:
            send(
                ret_out.at[c, rows_of(ep_to(d)), :], ret_in.at[c, rows_of(ep), :],
                s_out.at[3], s_r_r.at[c], {"ep": ep_to(d)})
        ret_in[c, rows_of(ep), :] = ret_out[c, rows_of(ep), :]

    cnt_all.wait_send()
    whole(z_in.at[:, pl.ds(0, others), :], s_out.at[0], s_z_r.at[0]).wait_send()
    n_x = sum(len(s) for s in shared)
    whole(rows.at[pl.ds(0, n_x)], s_out.at[1], s_x_r.at[0]).wait_send()
    whole(part_in.at[pl.ds(0, chunks * (n_tp - 1))], s_out.at[2], s_p_r.at[0]).wait_send()

    for c in range(chunks):
        whole(ret_in.at[c, pl.ds(0, others), :], s_out.at[3], s_r_r.at[c]).wait_recv()
        back = ret_in[c]
        out_ref[:, c * fc:(c + 1) * fc] = (
            jnp.dot(weight_hi[...], back, preferred_element_type=F32)
            + jnp.dot(weight_lo[...], back, preferred_element_type=F32)
        ).astype(BF16)

    whole(ret_in.at[:, pl.ds(0, others), :], s_out.at[3], s_r_r.at[0]).wait_send()


def per_device(tokens, selected, affinity, w_gate, w_up, w_down):
    n_ep = lax.axis_size("ep")
    n_tp = lax.axis_size("tp")
    n_tok, width = tokens.shape
    n_exp, group = selected.shape
    hidden = w_gate.shape[2]
    assert w_gate.shape[0] == 1 and n_exp == n_ep
    feats = width // n_tp
    chunks = max(1, feats // CHUNK)
    fc = feats // chunks
    n_z = chunks + len(plan(n_tp, chunks)[3])
    slots = n_ep * group
    live = slots // 2
    dma = pltpu.SemaphoreType.DMA
    any_spec = pl.BlockSpec(memory_space=pl.ANY)
    return pl.pallas_call(
        functools.partial(kernel, n_ep, n_tp, chunks),
        out_shape=pltpu.VMEM((n_tok, feats), BF16),
        in_specs=[any_spec] * 6,
        out_specs=pl.BlockSpec(memory_space=pltpu.VMEM),
        scratch_shapes=[
            pltpu.VMEM((n_tok, n_z * fc), BF16),
            pltpu.VMEM((n_exp, group), jnp.int32),
            pltpu.VMEM((n_exp, group), F32),
            pltpu.VMEM((width, 2 * hidden), BF16),
            pltpu.VMEM((chunks, hidden, n_tp * fc), BF16),
            pltpu.VMEM((slots, n_tok), F32),
            pltpu.VMEM((n_tok, slots), BF16),
            pltpu.VMEM((n_tok, slots), BF16),
            pltpu.VMEM((slots, live), BF16),
            pltpu.VMEM((live, slots), BF16),
            pltpu.VMEM((n_exp, 1, 128), F32),
            pltpu.VMEM((n_ep, 1, 128), F32),
            pltpu.VMEM((n_z, slots, fc), BF16),
            pltpu.VMEM((n_z, slots, fc), BF16),
            pltpu.VMEM((chunks * n_tp, live, fc), BF16),
            pltpu.VMEM((live, 2 * hidden), F32),
            pltpu.VMEM((live, hidden), BF16),
            pltpu.VMEM((chunks * n_tp, live, fc), BF16),
            pltpu.VMEM((chunks * n_tp, live, fc), BF16),
            pltpu.VMEM((chunks, slots, fc), BF16),
            pltpu.VMEM((chunks, slots, fc), BF16),
            dma((5,)),
            dma((2,)),
            dma((n_z,)),
            dma((chunks,)),
            dma((chunks,)),
            dma((chunks,)),
            dma((4,)),
        ],
        compiler_params=pltpu.CompilerParams(collective_id=0, has_side_effects=True),
    )(tokens, selected, affinity, w_gate, w_up, w_down)


def solution(mesh):
    placed = (
        P("ep", None),
        P(None, "ep"),
        P(None, "ep"),
        P("ep", None, "tp"),
        P("ep", None, "tp"),
        P("ep", "tp", None),
    )
    return jax.shard_map(
        per_device, mesh=mesh, in_specs=placed, out_specs=P("ep", "tp"), check_vma=False
    )
```

```python
import functools
import math

import jax
import jax.numpy as jnp
from jax import lax
from jax.experimental import pallas as pl
from jax.experimental.pallas import tpu as pltpu
from jax.sharding import PartitionSpec as P

MESH = pl.DeviceIdType.MESH
F32 = jnp.float32
BF16 = jnp.bfloat16
CHUNK = 128
OUT_EXTRA = 2
RET_EXTRA = 2
SIDE_AT = 2


def side_of(n):
    s = math.isqrt(n)
    while n % s:
        s -= 1
    return s


def plan(n_tp, chunks):
    width = side_of(n_tp)
    height = n_tp // width
    offsets = [(dy, dx) for dy in range(height) for dx in range(width)][1:]
    far = sorted(offsets, key=lambda o: -((o[0] > 0) + (o[1] > 0)))
    square = (height, width) == (2, 2)
    extra = list(range(chunks))[max(0, chunks - OUT_EXTRA):] if square and chunks > OUT_EXTRA else []
    back = list(range(RET_EXTRA)) if square and chunks > RET_EXTRA else []
    shared = [[o for o in far if not (c in extra and o == (1, 1))] for c in range(chunks)]
    reduced = [[o for o in far if not (c in back and o == (1, 1))] for c in range(chunks)]
    return width, height, far, extra, back, shared, reduced


def pieces_of(far, back, reduced, chunks):
    order = []
    for c in range(chunks):
        order += [(c, o) for o in reduced[c]]
        if c == 0:
            order += [(b, (1, 1)) for b in back]
    return order + [(c, (0, 0)) for c in range(chunks)]


def kernel(
    n_ep, n_tp, chunks,
    tok_hbm, sel_hbm, aff_hbm, wg_hbm, wu_hbm, wd_hbm, out_ref,
    tok, sel, aff, wgu, wd, onehot, weight_hi, weight_lo, expand, compact,
    cnt_out, cnt_in, z_out, z_in, rows, acc, hid, part_out, part_in, ret_out, ret_in,
    side_out, side_in,
    s_in, s_cnt, s_z_r, s_x_r, s_p_r, s_r_r, s_side_r, s_out,
):
    ep = lax.axis_index("ep")
    tp = lax.axis_index("tp")
    n_tok = tok.shape[0]
    n_exp, group = sel.shape
    fc = z_in.shape[2]
    feats = fc * chunks
    live = rows.shape[1]
    hidden = hid.shape[1]
    width, height, far, extra, back, shared, reduced = plan(n_tp, chunks)
    y, x = tp // width, lax.rem(tp, width)

    def tp_to(o):
        return lax.rem(y + o[0], height) * width + lax.rem(x + o[1], width)

    def tp_from(o):
        return lax.rem(y + height - o[0], height) * width + lax.rem(x + width - o[1], width)

    ep_order = list(range(n_ep - 1))
    high_half = ep // (n_ep // 2)

    def ep_to(i):
        down = n_ep - 1 - i
        down = down - jnp.where(down <= ep, 1, 0)
        up = i + jnp.where(i >= ep, 1, 0)
        return jnp.where(high_half > 0, up, down)

    def rows_of(i):
        return pl.ds(pl.multiple_of(i * group, group), group)

    def cols(k, c):
        return pl.ds(pl.multiple_of(k * feats + c * fc, 128), fc)

    def at(c, k):
        return c * n_tp + k

    z_chunks = [(c, (0, 0)) for c in range(chunks)] + [(c, (1, 1)) for c in extra]

    load_sel = pltpu.make_async_copy(sel_hbm, sel, s_in.at[0])
    load_sel.start()
    pltpu.make_async_copy(
        tok_hbm.at[:, pl.ds(pl.multiple_of(tp * feats, 128), feats)],
        tok.at[:, pl.ds(0, feats)], s_in.at[1]).start()
    if extra:
        first = extra[0] * fc
        start = pl.multiple_of(tp_to((1, 1)) * feats + first, 128)
        pltpu.make_async_copy(
            tok_hbm.at[:, pl.ds(start, feats - first)],
            tok.at[:, pl.ds(feats, feats - first)], s_in.at[1]).start()
    load_tok = pltpu.make_async_copy(tok, tok, s_in.at[1])

    barrier = pltpu.get_barrier_semaphore()
    for d in ep_order:
        pl.semaphore_signal(barrier, inc=1, device_id={"ep": ep_to(d)}, device_id_type=MESH)
    for o in far:
        pl.semaphore_signal(barrier, inc=1, device_id={"tp": tp_to(o)}, device_id_type=MESH)

    load_aff = pltpu.make_async_copy(aff_hbm, aff, s_in.at[2])
    load_aff.start()

    load_sel.wait()
    picked = sel[...].astype(F32)
    count = jnp.sum(jnp.where(picked >= 0, 1.0, 0.0), axis=1, keepdims=True)
    for e in range(n_exp):
        cnt_out[e] = jnp.broadcast_to(count[e:e + 1, :], (1, 128))
    picked_t = jnp.transpose(picked)
    token_lane = lax.broadcasted_iota(jnp.int32, (group, n_tok), 1).astype(F32)
    for e in range(n_exp):
        onehot[pl.ds(e * group, group), :] = jnp.where(
            picked_t[:, e:e + 1] == token_lane, 1.0, 0.0)
    load_tok.wait()
    pick = onehot[...].astype(BF16)

    def gather(i):
        z_out[i] = jnp.dot(
            pick, tok[:, i * fc:(i + 1) * fc], preferred_element_type=F32).astype(BF16)
        z_in[i, rows_of(ep), :] = z_out[i, rows_of(ep), :]

    gather(0)
    cnt_in[ep] = cnt_out[ep]

    pl.semaphore_wait(barrier, len(ep_order) + len(far))

    def send(src, dst, ss, rs, to):
        copy = pltpu.make_async_remote_copy(
            src_ref=src, dst_ref=dst, send_sem=ss, recv_sem=rs,
            device_id=to, device_id_type=MESH)
        copy.start()
        return copy

    others = (n_ep - 1) * group

    def whole(ref, ss, rs):
        return pltpu.make_async_remote_copy(
            src_ref=ref, dst_ref=ref, send_sem=ss, recv_sem=rs,
            device_id={"ep": ep_to(0)}, device_id_type=MESH)

    cnt_all = whole(cnt_in.at[pl.ds(0, n_ep - 1)], s_cnt.at[0], s_cnt.at[1])

    for d in ep_order:
        send(cnt_out.at[ep_to(d)], cnt_in.at[ep], s_cnt.at[0], s_cnt.at[1], {"ep": ep_to(d)})
    def spread_out(i):
        for d in ep_order:
            send(
                z_out.at[i, rows_of(ep_to(d)), :], z_in.at[i, rows_of(ep), :],
                s_out.at[0], s_z_r.at[i], {"ep": ep_to(d)})

    spread_out(0)
    for i in range(1, chunks):
        gather(i)
        spread_out(i)

    pltpu.make_async_copy(wg_hbm.at[0], wgu.at[:, pl.ds(0, hidden)], s_in.at[3]).start()
    pltpu.make_async_copy(wu_hbm.at[0], wgu.at[:, pl.ds(hidden, hidden)], s_in.at[3]).start()
    load_w = pltpu.make_async_copy(wgu, wgu, s_in.at[3])
    for i in range(chunks, len(z_chunks)):
        gather(i)
    for i, (c, o) in enumerate(pieces_of(far, back, reduced, chunks)):
        pltpu.make_async_copy(
            wd_hbm.at[0, :, cols(tp_to(o), c)], wd.at[:, pl.ds(i * fc, fc)], s_in.at[4]).start()
    load_d = pltpu.make_async_copy(wd, wd, s_in.at[4])

    load_aff.wait()
    aff_t = jnp.transpose(aff[...])
    for e in range(n_exp):
        block = pl.ds(e * group, group)
        onehot[block, :] = onehot[block, :] * aff_t[:, e:e + 1]
    weight = jnp.transpose(onehot[...])
    high = weight.astype(BF16)
    weight_hi[...] = high
    weight_lo[...] = (weight - high.astype(F32)).astype(BF16)

    load_w.wait()
    acc[...] = jnp.zeros_like(acc)

    cnt_all.wait_recv()
    lane = lax.broadcasted_iota(jnp.int32, (group, live), 1).astype(F32)
    row = lax.broadcasted_iota(jnp.int32, (group, live), 0).astype(F32)
    begin = jnp.zeros((group, live), F32)
    pieces = []
    for j in range(n_ep):
        n = jnp.broadcast_to(cnt_in[j, 0:1, 0:1], (group, live))
        pieces.append(jnp.where((lane - row == begin) & (row < n), 1.0, 0.0))
        begin = begin + n
    spread = jnp.concatenate(pieces, axis=0)
    expand[...] = spread.astype(BF16)
    compact[...] = jnp.transpose(spread).astype(BF16)

    def take(c, k):
        acc[...] += jnp.dot(rows[at(c, k)], wgu[cols(k, c), :], preferred_element_type=F32)

    def squeeze(i):
        c, o = z_chunks[i]
        whole(z_in.at[i, pl.ds(0, others), :], s_out.at[0], s_z_r.at[i]).wait_recv()
        rows[at(c, tp_to(o))] = jnp.dot(
            compact[...], z_in[i], preferred_element_type=F32).astype(BF16)

    def arrive(c):
        whole(rows.at[pl.ds(0, len(shared[c]))], s_out.at[1], s_x_r.at[c]).wait_recv()

    for c in range(chunks):
        squeeze(c)
        for o in shared[c]:
            send(
                rows.at[at(c, tp)], rows.at[at(c, tp)],
                s_out.at[1], s_x_r.at[c], {"tp": tp_to(o)})
        if 0 < c <= len(extra):
            spread_out(chunks + c - 1)
        take(c, tp)
    for c in range(chunks):
        if c in extra:
            squeeze(chunks + extra.index(c))
            take(c, tp_to((1, 1)))
        arrive(c)
        for o in shared[c]:
            take(c, tp_from(o))

    gate = acc[:, :hidden]
    up = acc[:, hidden:]
    hid[...] = (gate / (1.0 + jnp.exp(-gate)) * up).astype(BF16)
    load_d.wait()

    def give(i, value):
        ret_out[i] = jnp.dot(expand[...], value, preferred_element_type=F32).astype(BF16)
        for d in ep_order:
            send(
                ret_out.at[i, rows_of(ep_to(d)), :], ret_in.at[i, rows_of(ep), :],
                s_out.at[3], s_r_r.at[i], {"ep": ep_to(d)})
        ret_in[i, rows_of(ep), :] = ret_out[i, rows_of(ep), :]

    def combined(i):
        whole(ret_in.at[i, pl.ds(0, others), :], s_out.at[3], s_r_r.at[i]).wait_recv()
        value = ret_in[i]
        return (
            jnp.dot(weight_hi[...], value, preferred_element_type=F32)
            + jnp.dot(weight_lo[...], value, preferred_element_type=F32))

    order = pieces_of(far, back, reduced, chunks)
    step = max(1, 256 // fc)
    for i in range(0, len(order), step):
        some = order[i:i + step]
        value = jnp.dot(
            hid[...], wd[:, i * fc:(i + len(some)) * fc], preferred_element_type=F32).astype(BF16)
        for m, (c, o) in enumerate(some):
            k = tp_to(o)
            piece = value[:, m * fc:(m + 1) * fc]
            if o in reduced[c]:
                part_out[at(c, k)] = piece
                send(
                    part_out.at[at(c, k)], part_in.at[at(c, tp)],
                    s_out.at[2], s_p_r.at[c], {"tp": k})
            elif o == (0, 0):
                part_out[at(c, tp)] = piece
            else:
                give(chunks + back.index(c), piece)

    for c in range(chunks):
        total = part_out[at(c, tp)].astype(F32)
        whole(part_in.at[pl.ds(0, len(reduced[c]))], s_out.at[2], s_p_r.at[c]).wait_recv()
        for o in reduced[c]:
            total = total + part_in[at(c, tp_from(o))].astype(F32)
        give(c, total.astype(BF16))
        if c == min(SIDE_AT, chunks - 1):
            for b in range(len(back)):
                side_out[b] = combined(chunks + b).astype(BF16)
                send(
                    side_out.at[b], side_in.at[b],
                    s_out.at[4], s_side_r.at[b], {"tp": tp_to((1, 1))})

    cnt_all.wait_send()
    whole(z_in.at[:, pl.ds(0, others), :], s_out.at[0], s_z_r.at[0]).wait_send()
    n_x = sum(len(offsets) for offsets in shared)
    whole(rows.at[pl.ds(0, n_x)], s_out.at[1], s_x_r.at[0]).wait_send()
    n_p = sum(len(offsets) for offsets in reduced)
    whole(part_in.at[pl.ds(0, n_p)], s_out.at[2], s_p_r.at[0]).wait_send()

    plain = [c for c in range(chunks) if c not in back]
    for c in plain[:1] + back + plain[1:]:
        value = combined(c)
        if c in back:
            b = back.index(c)
            whole(side_in.at[b], s_out.at[4], s_side_r.at[b]).wait_recv()
            value = value + side_in[b].astype(F32)
        out_ref[:, c * fc:(c + 1) * fc] = value.astype(BF16)

    if back:
        whole(side_in, s_out.at[4], s_side_r.at[0]).wait_send()
    whole(ret_in.at[:, pl.ds(0, others), :], s_out.at[3], s_r_r.at[0]).wait_send()


def per_device(tokens, selected, affinity, w_gate, w_up, w_down):
    n_ep = lax.axis_size("ep")
    n_tp = lax.axis_size("tp")
    n_tok, width = tokens.shape
    n_exp, group = selected.shape
    hidden = w_gate.shape[2]
    assert w_gate.shape[0] == 1 and n_exp == n_ep
    feats = width // n_tp
    chunks = max(1, feats // CHUNK)
    fc = feats // chunks
    n_z = chunks + len(plan(n_tp, chunks)[3])
    n_back = len(plan(n_tp, chunks)[4])
    n_ret = chunks + n_back
    n_side = max(1, n_back)
    slots = n_ep * group
    live = slots // 2
    dma = pltpu.SemaphoreType.DMA
    any_spec = pl.BlockSpec(memory_space=pl.ANY)
    return pl.pallas_call(
        functools.partial(kernel, n_ep, n_tp, chunks),
        out_shape=pltpu.VMEM((n_tok, feats), BF16),
        in_specs=[any_spec] * 6,
        out_specs=pl.BlockSpec(memory_space=pltpu.VMEM),
        scratch_shapes=[
            pltpu.VMEM((n_tok, n_z * fc), BF16),
            pltpu.VMEM((n_exp, group), jnp.int32),
            pltpu.VMEM((n_exp, group), F32),
            pltpu.VMEM((width, 2 * hidden), BF16),
            pltpu.VMEM((hidden, width), BF16),
            pltpu.VMEM((slots, n_tok), F32),
            pltpu.VMEM((n_tok, slots), BF16),
            pltpu.VMEM((n_tok, slots), BF16),
            pltpu.VMEM((slots, live), BF16),
            pltpu.VMEM((live, slots), BF16),
            pltpu.VMEM((n_exp, 1, 128), F32),
            pltpu.VMEM((n_ep, 1, 128), F32),
            pltpu.VMEM((n_z, slots, fc), BF16),
            pltpu.VMEM((n_z, slots, fc), BF16),
            pltpu.VMEM((chunks * n_tp, live, fc), BF16),
            pltpu.VMEM((live, 2 * hidden), F32),
            pltpu.VMEM((live, hidden), BF16),
            pltpu.VMEM((chunks * n_tp, live, fc), BF16),
            pltpu.VMEM((chunks * n_tp, live, fc), BF16),
            pltpu.VMEM((n_ret, slots, fc), BF16),
            pltpu.VMEM((n_ret, slots, fc), BF16),
            pltpu.VMEM((n_side, n_tok, fc), BF16),
            pltpu.VMEM((n_side, n_tok, fc), BF16),
            dma((5,)),
            dma((2,)),
            dma((n_z,)),
            dma((chunks,)),
            dma((chunks,)),
            dma((n_ret,)),
            dma((n_side,)),
            dma((5,)),
        ],
        compiler_params=pltpu.CompilerParams(collective_id=0, has_side_effects=True),
    )(tokens, selected, affinity, w_gate, w_up, w_down)


def solution(mesh):
    placed = (
        P("ep", None),
        P(None, "ep"),
        P(None, "ep"),
        P("ep", None, "tp"),
        P("ep", None, "tp"),
        P("ep", "tp", None),
    )
    return jax.shard_map(
        per_device, mesh=mesh, in_specs=placed, out_specs=P("ep", "tp"), check_vma=False
    )
```

```python
import functools
import math

import jax
import jax.numpy as jnp
from jax import lax
from jax.experimental import pallas as pl
from jax.experimental.pallas import tpu as pltpu
from jax.sharding import PartitionSpec as P

MESH = pl.DeviceIdType.MESH
F32 = jnp.float32
BF16 = jnp.bfloat16
CHUNK = 128
OUT_EXTRA = 2
BACK = (0, 1)
SIDE_AT = 2


def side_of(n):
    s = math.isqrt(n)
    while n % s:
        s -= 1
    return s


def plan(n_tp, chunks):
    width = side_of(n_tp)
    height = n_tp // width
    offsets = [(dy, dx) for dy in range(height) for dx in range(width)][1:]
    far = sorted(offsets, key=lambda o: -((o[0] > 0) + (o[1] > 0)))
    square = (height, width) == (2, 2)
    extra = list(range(chunks))[max(0, chunks - OUT_EXTRA):] if square and chunks > OUT_EXTRA else []
    back = [c for c in BACK if square and chunks > max(BACK)]
    shared = [[o for o in far if not (c in extra and o == (1, 1))] for c in range(chunks)]
    reduced = [[o for o in far if not (c in back and o == (1, 1))] for c in range(chunks)]
    return width, height, far, extra, back, shared, reduced


def pieces_of(far, back, reduced, chunks):
    order = []
    for c in range(chunks):
        order += [(c, o) for o in reduced[c]]
        if c == 0:
            order += [(b, (1, 1)) for b in back]
    return order + [(c, (0, 0)) for c in range(chunks)]


def run(
    n_ep, n_tp, chunks,
    tok_hbm, sel_hbm, aff_hbm, wg_hbm, wu_hbm, wd_hbm, out_ref,
    tok, sel, aff, wgu, wd, onehot, weight_hi, weight_lo, expand, compact,
    cnt_out, cnt_in, z_out, z_in, rows, acc, hid, part_out, part_in, ret_out, ret_in,
    side_out, side_in,
    s_in, s_cnt, s_z_r, s_x_r, s_p_r, s_r_r, s_side_r, s_out,
):
    ep = lax.axis_index("ep")
    tp = lax.axis_index("tp")
    n_tok = tok.shape[0]
    n_exp, group = sel.shape
    fc = z_in.shape[2]
    feats = fc * chunks
    live = rows.shape[1]
    hidden = hid.shape[1]
    width, height, far, extra, back, shared, reduced = plan(n_tp, chunks)
    y, x = tp // width, lax.rem(tp, width)

    def tp_to(o):
        return lax.rem(y + o[0], height) * width + lax.rem(x + o[1], width)

    def tp_from(o):
        return lax.rem(y + height - o[0], height) * width + lax.rem(x + width - o[1], width)

    ep_order = list(range(n_ep - 1))
    high_half = ep // (n_ep // 2)

    def ep_to(i):
        down = n_ep - 1 - i
        down = down - jnp.where(down <= ep, 1, 0)
        up = i + jnp.where(i >= ep, 1, 0)
        return jnp.where(high_half > 0, up, down)

    def rows_of(i):
        return pl.ds(pl.multiple_of(i * group, group), group)

    def cols(k, c):
        return pl.ds(pl.multiple_of(k * feats + c * fc, 128), fc)

    def at(c, k):
        return c * n_tp + k

    z_chunks = [(c, (0, 0)) for c in range(chunks)] + [(c, (1, 1)) for c in extra]

    load_sel = pltpu.make_async_copy(sel_hbm, sel, s_in.at[0])
    load_sel.start()
    pltpu.make_async_copy(
        tok_hbm.at[:, pl.ds(pl.multiple_of(tp * feats, 128), feats)],
        tok.at[:, pl.ds(0, feats)], s_in.at[1]).start()
    if extra:
        first = extra[0] * fc
        start = pl.multiple_of(tp_to((1, 1)) * feats + first, 128)
        pltpu.make_async_copy(
            tok_hbm.at[:, pl.ds(start, feats - first)],
            tok.at[:, pl.ds(feats, feats - first)], s_in.at[1]).start()
    load_tok = pltpu.make_async_copy(tok, tok, s_in.at[1])

    barrier = pltpu.get_barrier_semaphore()
    for d in ep_order:
        pl.semaphore_signal(barrier, inc=1, device_id={"ep": ep_to(d)}, device_id_type=MESH)
    for o in far:
        pl.semaphore_signal(barrier, inc=1, device_id={"tp": tp_to(o)}, device_id_type=MESH)

    load_aff = pltpu.make_async_copy(aff_hbm, aff, s_in.at[2])
    load_aff.start()

    load_sel.wait()
    picked = sel[...].astype(F32)
    count = jnp.sum(jnp.where(picked >= 0, 1.0, 0.0), axis=1, keepdims=True)
    for e in range(n_exp):
        cnt_out[e] = jnp.broadcast_to(count[e:e + 1, :], (1, 128))
    picked_t = jnp.transpose(picked)
    token_lane = lax.broadcasted_iota(jnp.int32, (group, n_tok), 1).astype(F32)
    for e in range(n_exp):
        onehot[pl.ds(e * group, group), :] = jnp.where(
            picked_t[:, e:e + 1] == token_lane, 1.0, 0.0)
    load_tok.wait()
    pick = onehot[...].astype(BF16)

    def gather(i):
        z_out[i] = jnp.dot(
            pick, tok[:, i * fc:(i + 1) * fc], preferred_element_type=F32).astype(BF16)
        z_in[i, rows_of(ep), :] = z_out[i, rows_of(ep), :]

    gather(0)
    cnt_in[ep] = cnt_out[ep]

    pl.semaphore_wait(barrier, len(ep_order) + len(far))

    def send(src, dst, ss, rs, to):
        copy = pltpu.make_async_remote_copy(
            src_ref=src, dst_ref=dst, send_sem=ss, recv_sem=rs,
            device_id=to, device_id_type=MESH)
        copy.start()
        return copy

    others = (n_ep - 1) * group

    def whole(ref, ss, rs):
        return pltpu.make_async_remote_copy(
            src_ref=ref, dst_ref=ref, send_sem=ss, recv_sem=rs,
            device_id={"ep": ep_to(0)}, device_id_type=MESH)

    cnt_all = whole(cnt_in.at[pl.ds(0, n_ep - 1)], s_cnt.at[0], s_cnt.at[1])

    for d in ep_order:
        send(cnt_out.at[ep_to(d)], cnt_in.at[ep], s_cnt.at[0], s_cnt.at[1], {"ep": ep_to(d)})
    def spread_out(i):
        for d in ep_order:
            send(
                z_out.at[i, rows_of(ep_to(d)), :], z_in.at[i, rows_of(ep), :],
                s_out.at[0], s_z_r.at[i], {"ep": ep_to(d)})

    spread_out(0)
    for i in range(1, chunks):
        gather(i)
        spread_out(i)

    pltpu.make_async_copy(wg_hbm.at[0], wgu.at[:, pl.ds(0, hidden)], s_in.at[3]).start()
    pltpu.make_async_copy(wu_hbm.at[0], wgu.at[:, pl.ds(hidden, hidden)], s_in.at[3]).start()
    load_w = pltpu.make_async_copy(wgu, wgu, s_in.at[3])
    for i in range(chunks, len(z_chunks)):
        gather(i)
    for i, (c, o) in enumerate(pieces_of(far, back, reduced, chunks)):
        pltpu.make_async_copy(
            wd_hbm.at[0, :, cols(tp_to(o), c)], wd.at[:, pl.ds(i * fc, fc)], s_in.at[4]).start()
    load_d = pltpu.make_async_copy(wd, wd, s_in.at[4])

    load_aff.wait()
    aff_t = jnp.transpose(aff[...])
    for e in range(n_exp):
        block = pl.ds(e * group, group)
        onehot[block, :] = onehot[block, :] * aff_t[:, e:e + 1]
    weight = jnp.transpose(onehot[...])
    high = weight.astype(BF16)
    weight_hi[...] = high
    weight_lo[...] = (weight - high.astype(F32)).astype(BF16)

    load_w.wait()
    acc[...] = jnp.zeros_like(acc)

    cnt_all.wait_recv()
    lane = lax.broadcasted_iota(jnp.int32, (group, live), 1).astype(F32)
    row = lax.broadcasted_iota(jnp.int32, (group, live), 0).astype(F32)
    begin = jnp.zeros((group, live), F32)
    pieces = []
    for j in range(n_ep):
        n = jnp.broadcast_to(cnt_in[j, 0:1, 0:1], (group, live))
        pieces.append(jnp.where((lane - row == begin) & (row < n), 1.0, 0.0))
        begin = begin + n
    spread = jnp.concatenate(pieces, axis=0)
    expand[...] = spread.astype(BF16)
    compact[...] = jnp.transpose(spread).astype(BF16)

    def take(c, k):
        acc[...] += jnp.dot(rows[at(c, k)], wgu[cols(k, c), :], preferred_element_type=F32)

    def squeeze(i):
        c, o = z_chunks[i]
        whole(z_in.at[i, pl.ds(0, others), :], s_out.at[0], s_z_r.at[i]).wait_recv()
        rows[at(c, tp_to(o))] = jnp.dot(
            compact[...], z_in[i], preferred_element_type=F32).astype(BF16)

    def arrive(c):
        whole(rows.at[pl.ds(0, len(shared[c]))], s_out.at[1], s_x_r.at[c]).wait_recv()

    for c in range(chunks):
        squeeze(c)
        for o in shared[c]:
            send(
                rows.at[at(c, tp)], rows.at[at(c, tp)],
                s_out.at[1], s_x_r.at[c], {"tp": tp_to(o)})
        if c == 1:
            for i in range(len(extra)):
                spread_out(chunks + i)
        take(c, tp)
    for c in range(chunks):
        if c in extra:
            squeeze(chunks + extra.index(c))
            take(c, tp_to((1, 1)))
        arrive(c)
        for o in shared[c]:
            take(c, tp_from(o))

    gate = acc[:, :hidden]
    up = acc[:, hidden:]
    hid[...] = (gate / (1.0 + jnp.exp(-gate)) * up).astype(BF16)
    load_d.wait()

    def give(i, value):
        ret_out[i] = jnp.dot(expand[...], value, preferred_element_type=F32).astype(BF16)
        for d in ep_order:
            send(
                ret_out.at[i, rows_of(ep_to(d)), :], ret_in.at[i, rows_of(ep), :],
                s_out.at[3], s_r_r.at[i], {"ep": ep_to(d)})
        ret_in[i, rows_of(ep), :] = ret_out[i, rows_of(ep), :]

    def combined(i):
        whole(ret_in.at[i, pl.ds(0, others), :], s_out.at[3], s_r_r.at[i]).wait_recv()
        value = ret_in[i]
        return (
            jnp.dot(weight_hi[...], value, preferred_element_type=F32)
            + jnp.dot(weight_lo[...], value, preferred_element_type=F32))

    order = pieces_of(far, back, reduced, chunks)
    step = max(1, 256 // fc)
    for i in range(0, len(order), step):
        some = order[i:i + step]
        value = jnp.dot(
            hid[...], wd[:, i * fc:(i + len(some)) * fc], preferred_element_type=F32).astype(BF16)
        for m, (c, o) in enumerate(some):
            k = tp_to(o)
            piece = value[:, m * fc:(m + 1) * fc]
            if o in reduced[c]:
                part_out[at(c, k)] = piece
                send(
                    part_out.at[at(c, k)], part_in.at[at(c, tp)],
                    s_out.at[2], s_p_r.at[c], {"tp": k})
            elif o == (0, 0):
                part_out[at(c, tp)] = piece
            else:
                give(chunks + back.index(c), piece)

    for c in range(chunks):
        total = part_out[at(c, tp)].astype(F32)
        whole(part_in.at[pl.ds(0, len(reduced[c]))], s_out.at[2], s_p_r.at[c]).wait_recv()
        for o in reduced[c]:
            total = total + part_in[at(c, tp_from(o))].astype(F32)
        give(c, total.astype(BF16))
        if c == min(SIDE_AT, chunks - 1):
            for b in range(len(back)):
                side_out[b] = combined(chunks + b).astype(BF16)
                send(
                    side_out.at[b], side_in.at[b],
                    s_out.at[4], s_side_r.at[b], {"tp": tp_to((1, 1))})

    cnt_all.wait_send()
    whole(z_in.at[:, pl.ds(0, others), :], s_out.at[0], s_z_r.at[0]).wait_send()
    n_x = sum(len(offsets) for offsets in shared)
    whole(rows.at[pl.ds(0, n_x)], s_out.at[1], s_x_r.at[0]).wait_send()
    n_p = sum(len(offsets) for offsets in reduced)
    whole(part_in.at[pl.ds(0, n_p)], s_out.at[2], s_p_r.at[0]).wait_send()

    for c in [1, 0, *range(2, chunks)] if back else range(chunks):
        value = combined(c)
        if c in back:
            b = back.index(c)
            whole(side_in.at[b], s_out.at[4], s_side_r.at[b]).wait_recv()
            value = value + side_in[b].astype(F32)
        out_ref[:, c * fc:(c + 1) * fc] = value.astype(BF16)

    if back:
        whole(side_in, s_out.at[4], s_side_r.at[0]).wait_send()
    whole(ret_in.at[:, pl.ds(0, others), :], s_out.at[3], s_r_r.at[0]).wait_send()


def kernel(n_ep, n_tp, chunks, *refs):
    n_z = chunks + len(plan(n_tp, chunks)[3])
    n_back = len(plan(n_tp, chunks)[4])
    dma = pltpu.SemaphoreType.DMA
    pl.run_scoped(
        functools.partial(run, n_ep, n_tp, chunks, *refs),
        dma((5,)), dma((2,)), dma((n_z,)), dma((chunks,)), dma((chunks,)), dma((chunks + n_back,)),
        dma((max(1, n_back),)), dma((5,)))


def per_device(tokens, selected, affinity, w_gate, w_up, w_down):
    n_ep = lax.axis_size("ep")
    n_tp = lax.axis_size("tp")
    n_tok, width = tokens.shape
    n_exp, group = selected.shape
    hidden = w_gate.shape[2]
    assert w_gate.shape[0] == 1 and n_exp == n_ep
    feats = width // n_tp
    chunks = max(1, feats // CHUNK)
    fc = feats // chunks
    n_z = chunks + len(plan(n_tp, chunks)[3])
    n_back = len(plan(n_tp, chunks)[4])
    n_ret = chunks + n_back
    n_side = max(1, n_back)
    slots = n_ep * group
    live = slots // 2
    any_spec = pl.BlockSpec(memory_space=pl.ANY)
    return pl.pallas_call(
        functools.partial(kernel, n_ep, n_tp, chunks),
        out_shape=pltpu.VMEM((n_tok, feats), BF16),
        in_specs=[any_spec] * 6,
        out_specs=pl.BlockSpec(memory_space=pltpu.VMEM),
        scratch_shapes=[
            pltpu.VMEM((n_tok, n_z * fc), BF16),
            pltpu.VMEM((n_exp, group), jnp.int32),
            pltpu.VMEM((n_exp, group), F32),
            pltpu.VMEM((width, 2 * hidden), BF16),
            pltpu.VMEM((hidden, width), BF16),
            pltpu.VMEM((slots, n_tok), F32),
            pltpu.VMEM((n_tok, slots), BF16),
            pltpu.VMEM((n_tok, slots), BF16),
            pltpu.VMEM((slots, live), BF16),
            pltpu.VMEM((live, slots), BF16),
            pltpu.VMEM((n_exp, 1, 128), F32),
            pltpu.VMEM((n_ep, 1, 128), F32),
            pltpu.VMEM((n_z, slots, fc), BF16),
            pltpu.VMEM((n_z, slots, fc), BF16),
            pltpu.VMEM((chunks * n_tp, live, fc), BF16),
            pltpu.VMEM((live, 2 * hidden), F32),
            pltpu.VMEM((live, hidden), BF16),
            pltpu.VMEM((chunks * n_tp, live, fc), BF16),
            pltpu.VMEM((chunks * n_tp, live, fc), BF16),
            pltpu.VMEM((n_ret, slots, fc), BF16),
            pltpu.VMEM((n_ret, slots, fc), BF16),
            pltpu.VMEM((n_side, n_tok, fc), BF16),
            pltpu.VMEM((n_side, n_tok, fc), BF16),
        ],
        compiler_params=pltpu.CompilerParams(collective_id=0, has_side_effects=True),
    )(tokens, selected, affinity, w_gate, w_up, w_down)


def solution(mesh):
    placed = (
        P("ep", None),
        P(None, "ep"),
        P(None, "ep"),
        P("ep", None, "tp"),
        P("ep", None, "tp"),
        P("ep", "tp", None),
    )
    return jax.shard_map(
        per_device, mesh=mesh, in_specs=placed, out_specs=P("ep", "tp"), check_vma=False
    )
```

```python
import functools
import math

import jax
import jax.numpy as jnp
from jax import lax
from jax.experimental import pallas as pl
from jax.experimental.pallas import tpu as pltpu
from jax.sharding import PartitionSpec as P

MESH = pl.DeviceIdType.MESH
F32 = jnp.float32
BF16 = jnp.bfloat16
CHUNK = 128
OUT_EXTRA = 1
OUT_SPLIT = 2
SPLIT_CORE = 0
BACK = (0, 1)
SIDE_AT = 2


def side_of(n):
    s = math.isqrt(n)
    while n % s:
        s -= 1
    return s


def plan(n_tp, chunks):
    width = side_of(n_tp)
    height = n_tp // width
    offsets = [(dy, dx) for dy in range(height) for dx in range(width)][1:]
    far = sorted(offsets, key=lambda o: -((o[0] > 0) + (o[1] > 0)))
    square = (height, width) == (2, 2)
    both = chunks - OUT_EXTRA
    some = both - OUT_SPLIT
    extra = list(range(some, chunks)) if square and some > 0 else []
    split = list(range(some, both)) if square and some > 0 else []
    back = [c for c in BACK if square and chunks > max(BACK)]
    shared = [
        [o for o in far if not (c in extra and c not in split and o == (1, 1))] for c in range(chunks)]
    reduced = [[o for o in far if not (c in back and o == (1, 1))] for c in range(chunks)]
    return width, height, far, extra, split, back, shared, reduced


def pieces_of(far, back, reduced, chunks):
    order = []
    for c in range(chunks):
        order += [(c, o) for o in reduced[c]]
        if c == 0:
            order += [(b, (1, 1)) for b in back]
    return order + [(c, (0, 0)) for c in range(chunks)]


def run(
    n_ep, n_tp, chunks,
    tok_hbm, sel_hbm, aff_hbm, wg_hbm, wu_hbm, wd_hbm, out_ref,
    tok, sel, aff, wgu, wd, onehot, weight_hi, weight_lo, expand, compact,
    cnt_out, cnt_in, z_out, z_in, rows, acc, hid, part_out, part_in, ret_out, ret_in,
    side_out, side_in,
    s_in, s_cnt, s_z_r, s_x_r, s_p_r, s_r_r, s_side_r, s_out,
):
    ep = lax.axis_index("ep")
    tp = lax.axis_index("tp")
    n_tok = tok.shape[0]
    n_exp, group = sel.shape
    fc = z_in.shape[2]
    feats = fc * chunks
    live = rows.shape[1]
    hidden = hid.shape[1]
    width, height, far, extra, split, back, shared, reduced = plan(n_tp, chunks)
    over_ep = lax.rem(ep, 2) == SPLIT_CORE
    over_tp = lax.rem(ep, 2) != SPLIT_CORE
    y, x = tp // width, lax.rem(tp, width)

    def tp_to(o):
        return lax.rem(y + o[0], height) * width + lax.rem(x + o[1], width)

    def tp_from(o):
        return lax.rem(y + height - o[0], height) * width + lax.rem(x + width - o[1], width)

    ep_order = list(range(n_ep - 1))
    high_half = ep // (n_ep // 2)

    def ep_to(i):
        down = n_ep - 1 - i
        down = down - jnp.where(down <= ep, 1, 0)
        up = i + jnp.where(i >= ep, 1, 0)
        return jnp.where(high_half > 0, up, down)

    def rows_of(i):
        return pl.ds(pl.multiple_of(i * group, group), group)

    def cols(k, c):
        return pl.ds(pl.multiple_of(k * feats + c * fc, 128), fc)

    def at(c, k):
        return c * n_tp + k

    z_chunks = [(c, (0, 0)) for c in range(chunks)] + [(c, (1, 1)) for c in extra]

    load_sel = pltpu.make_async_copy(sel_hbm, sel, s_in.at[0])
    load_sel.start()
    pltpu.make_async_copy(
        tok_hbm.at[:, pl.ds(pl.multiple_of(tp * feats, 128), feats)],
        tok.at[:, pl.ds(0, feats)], s_in.at[1]).start()
    if extra:
        first = extra[0] * fc
        start = pl.multiple_of(tp_to((1, 1)) * feats + first, 128)
        pltpu.make_async_copy(
            tok_hbm.at[:, pl.ds(start, feats - first)],
            tok.at[:, pl.ds(feats, feats - first)], s_in.at[1]).start()
    load_tok = pltpu.make_async_copy(tok, tok, s_in.at[1])

    barrier = pltpu.get_barrier_semaphore()
    for d in ep_order:
        pl.semaphore_signal(barrier, inc=1, device_id={"ep": ep_to(d)}, device_id_type=MESH)
    for o in far:
        pl.semaphore_signal(barrier, inc=1, device_id={"tp": tp_to(o)}, device_id_type=MESH)

    load_aff = pltpu.make_async_copy(aff_hbm, aff, s_in.at[2])
    load_aff.start()

    load_sel.wait()
    picked = sel[...].astype(F32)
    count = jnp.sum(jnp.where(picked >= 0, 1.0, 0.0), axis=1, keepdims=True)
    for e in range(n_exp):
        cnt_out[e] = jnp.broadcast_to(count[e:e + 1, :], (1, 128))
    picked_t = jnp.transpose(picked)
    token_lane = lax.broadcasted_iota(jnp.int32, (group, n_tok), 1).astype(F32)
    for e in range(n_exp):
        onehot[pl.ds(e * group, group), :] = jnp.where(
            picked_t[:, e:e + 1] == token_lane, 1.0, 0.0)
    load_tok.wait()
    pick = onehot[...].astype(BF16)

    def gather(i):
        z_out[i] = jnp.dot(
            pick, tok[:, i * fc:(i + 1) * fc], preferred_element_type=F32).astype(BF16)
        z_in[i, rows_of(ep), :] = z_out[i, rows_of(ep), :]

    gather(0)
    cnt_in[ep] = cnt_out[ep]

    pl.semaphore_wait(barrier, len(ep_order) + len(far))

    def send(src, dst, ss, rs, to):
        copy = pltpu.make_async_remote_copy(
            src_ref=src, dst_ref=dst, send_sem=ss, recv_sem=rs,
            device_id=to, device_id_type=MESH)
        copy.start()
        return copy

    others = (n_ep - 1) * group

    def whole(ref, ss, rs):
        return pltpu.make_async_remote_copy(
            src_ref=ref, dst_ref=ref, send_sem=ss, recv_sem=rs,
            device_id={"ep": ep_to(0)}, device_id_type=MESH)

    cnt_all = whole(cnt_in.at[pl.ds(0, n_ep - 1)], s_cnt.at[0], s_cnt.at[1])

    for d in ep_order:
        send(cnt_out.at[ep_to(d)], cnt_in.at[ep], s_cnt.at[0], s_cnt.at[1], {"ep": ep_to(d)})
    def spread_some(i):
        for j in range(n_ep // 2):
            e = 2 * jnp.where(high_half > 0, j, n_ep // 2 - 1 - j) + SPLIT_CORE

            @pl.when(e != ep)
            def _(e=e):
                send(
                    z_out.at[i, rows_of(e), :], z_in.at[i, rows_of(ep), :],
                    s_out.at[0], s_z_r.at[i], {"ep": e})

    def spread_out(i):
        for d in ep_order:
            send(
                z_out.at[i, rows_of(ep_to(d)), :], z_in.at[i, rows_of(ep), :],
                s_out.at[0], s_z_r.at[i], {"ep": ep_to(d)})

    spread_out(0)
    for i in range(1, chunks):
        gather(i)
        spread_out(i)

    pltpu.make_async_copy(wg_hbm.at[0], wgu.at[:, pl.ds(0, hidden)], s_in.at[3]).start()
    pltpu.make_async_copy(wu_hbm.at[0], wgu.at[:, pl.ds(hidden, hidden)], s_in.at[3]).start()
    load_w = pltpu.make_async_copy(wgu, wgu, s_in.at[3])
    for i in range(chunks, len(z_chunks)):
        gather(i)
    for i, (c, o) in enumerate(pieces_of(far, back, reduced, chunks)):
        pltpu.make_async_copy(
            wd_hbm.at[0, :, cols(tp_to(o), c)], wd.at[:, pl.ds(i * fc, fc)], s_in.at[4]).start()
    load_d = pltpu.make_async_copy(wd, wd, s_in.at[4])

    load_aff.wait()
    aff_t = jnp.transpose(aff[...])
    for e in range(n_exp):
        block = pl.ds(e * group, group)
        onehot[block, :] = onehot[block, :] * aff_t[:, e:e + 1]
    weight = jnp.transpose(onehot[...])
    high = weight.astype(BF16)
    weight_hi[...] = high
    weight_lo[...] = (weight - high.astype(F32)).astype(BF16)

    load_w.wait()
    acc[...] = jnp.zeros_like(acc)

    cnt_all.wait_recv()
    lane = lax.broadcasted_iota(jnp.int32, (group, live), 1).astype(F32)
    row = lax.broadcasted_iota(jnp.int32, (group, live), 0).astype(F32)
    begin = jnp.zeros((group, live), F32)
    pieces = []
    for j in range(n_ep):
        n = jnp.broadcast_to(cnt_in[j, 0:1, 0:1], (group, live))
        pieces.append(jnp.where((lane - row == begin) & (row < n), 1.0, 0.0))
        begin = begin + n
    spread = jnp.concatenate(pieces, axis=0)
    expand[...] = spread.astype(BF16)
    compact[...] = jnp.transpose(spread).astype(BF16)

    def take(c, k):
        acc[...] += jnp.dot(rows[at(c, k)], wgu[cols(k, c), :], preferred_element_type=F32)

    def squeeze(i):
        c, o = z_chunks[i]
        whole(z_in.at[i, pl.ds(0, others), :], s_out.at[0], s_z_r.at[i]).wait_recv()
        rows[at(c, tp_to(o))] = jnp.dot(
            compact[...], z_in[i], preferred_element_type=F32).astype(BF16)

    def shared_in(c, n):
        return whole(rows.at[pl.ds(0, n)], s_out.at[1], s_x_r.at[c])

    for c in range(chunks):
        squeeze(c)
        for o in shared[c]:
            def share(c=c, o=o):
                send(
                    rows.at[at(c, tp)], rows.at[at(c, tp)],
                    s_out.at[1], s_x_r.at[c], {"tp": tp_to(o)})

            if c in split and o == (1, 1):
                pl.when(over_tp)(share)
            else:
                share()
        if c == 1:
            for i, b in enumerate(extra):
                if b in split:
                    spread_some(chunks + i)
                else:
                    spread_out(chunks + i)
        take(c, tp)
    for c in range(chunks):
        def direct(c=c):
            squeeze(chunks + extra.index(c))
            take(c, tp_to((1, 1)))

        if c in split:
            @pl.when(over_ep)
            def _(c=c):
                direct()
                shared_in(c, len(shared[c]) - 1).wait_recv()

            @pl.when(over_tp)
            def _(c=c):
                shared_in(c, len(shared[c])).wait_recv()
                take(c, tp_from((1, 1)))
        else:
            if c in extra:
                direct()
            shared_in(c, len(shared[c])).wait_recv()
        for o in shared[c]:
            if not (c in split and o == (1, 1)):
                take(c, tp_from(o))

    gate = acc[:, :hidden]
    up = acc[:, hidden:]
    hid[...] = (gate / (1.0 + jnp.exp(-gate)) * up).astype(BF16)
    load_d.wait()

    def give(i, value):
        ret_out[i] = jnp.dot(expand[...], value, preferred_element_type=F32).astype(BF16)
        for d in ep_order:
            send(
                ret_out.at[i, rows_of(ep_to(d)), :], ret_in.at[i, rows_of(ep), :],
                s_out.at[3], s_r_r.at[i], {"ep": ep_to(d)})
        ret_in[i, rows_of(ep), :] = ret_out[i, rows_of(ep), :]

    def combined(i):
        whole(ret_in.at[i, pl.ds(0, others), :], s_out.at[3], s_r_r.at[i]).wait_recv()
        value = ret_in[i]
        return (
            jnp.dot(weight_hi[...], value, preferred_element_type=F32)
            + jnp.dot(weight_lo[...], value, preferred_element_type=F32))

    order = pieces_of(far, back, reduced, chunks)
    step = max(1, 256 // fc)
    for i in range(0, len(order), step):
        some = order[i:i + step]
        value = jnp.dot(
            hid[...], wd[:, i * fc:(i + len(some)) * fc], preferred_element_type=F32).astype(BF16)
        for m, (c, o) in enumerate(some):
            k = tp_to(o)
            piece = value[:, m * fc:(m + 1) * fc]
            if o in reduced[c]:
                part_out[at(c, k)] = piece
                send(
                    part_out.at[at(c, k)], part_in.at[at(c, tp)],
                    s_out.at[2], s_p_r.at[c], {"tp": k})
            elif o == (0, 0):
                part_out[at(c, tp)] = piece
            else:
                give(chunks + back.index(c), piece)

    for c in range(chunks):
        total = part_out[at(c, tp)].astype(F32)
        whole(part_in.at[pl.ds(0, len(reduced[c]))], s_out.at[2], s_p_r.at[c]).wait_recv()
        for o in reduced[c]:
            total = total + part_in[at(c, tp_from(o))].astype(F32)
        give(c, total.astype(BF16))
        if c == min(SIDE_AT, chunks - 1):
            for b in range(len(back)):
                side_out[b] = combined(chunks + b).astype(BF16)
                send(
                    side_out.at[b], side_in.at[b],
                    s_out.at[4], s_side_r.at[b], {"tp": tp_to((1, 1))})

    cnt_all.wait_send()
    n_all = len(z_chunks) - len(split)
    whole(z_in.at[pl.ds(0, n_all), pl.ds(0, others), :], s_out.at[0], s_z_r.at[0]).wait_send()
    n_x = sum(len(offsets) for offsets in shared)
    if split:
        def some_out(n):
            return whole(
                z_in.at[pl.ds(0, len(split)), pl.ds(0, n * group), :], s_out.at[0], s_z_r.at[0])

        @pl.when(over_ep)
        def _():
            some_out(n_ep // 2 - 1).wait_send()
            shared_in(0, n_x - len(split)).wait_send()

        @pl.when(over_tp)
        def _():
            some_out(n_ep // 2).wait_send()
            shared_in(0, n_x).wait_send()
    else:
        shared_in(0, n_x).wait_send()
    n_p = sum(len(offsets) for offsets in reduced)
    whole(part_in.at[pl.ds(0, n_p)], s_out.at[2], s_p_r.at[0]).wait_send()

    for c in [1, 0, *range(2, chunks)] if back else range(chunks):
        value = combined(c)
        if c in back:
            b = back.index(c)
            whole(side_in.at[b], s_out.at[4], s_side_r.at[b]).wait_recv()
            value = value + side_in[b].astype(F32)
        out_ref[:, c * fc:(c + 1) * fc] = value.astype(BF16)

    if back:
        whole(side_in, s_out.at[4], s_side_r.at[0]).wait_send()
    whole(ret_in.at[:, pl.ds(0, others), :], s_out.at[3], s_r_r.at[0]).wait_send()


def kernel(n_ep, n_tp, chunks, *refs):
    n_z = chunks + len(plan(n_tp, chunks)[3])
    n_back = len(plan(n_tp, chunks)[5])
    dma = pltpu.SemaphoreType.DMA
    pl.run_scoped(
        functools.partial(run, n_ep, n_tp, chunks, *refs),
        dma((5,)), dma((2,)), dma((n_z,)), dma((chunks,)), dma((chunks,)), dma((chunks + n_back,)),
        dma((max(1, n_back),)), dma((5,)))


def per_device(tokens, selected, affinity, w_gate, w_up, w_down):
    n_ep = lax.axis_size("ep")
    n_tp = lax.axis_size("tp")
    n_tok, width = tokens.shape
    n_exp, group = selected.shape
    hidden = w_gate.shape[2]
    assert w_gate.shape[0] == 1 and n_exp == n_ep
    feats = width // n_tp
    chunks = max(1, feats // CHUNK)
    fc = feats // chunks
    n_z = chunks + len(plan(n_tp, chunks)[3])
    n_back = len(plan(n_tp, chunks)[5])
    n_ret = chunks + n_back
    n_side = max(1, n_back)
    slots = n_ep * group
    live = slots // 2
    any_spec = pl.BlockSpec(memory_space=pl.ANY)
    return pl.pallas_call(
        functools.partial(kernel, n_ep, n_tp, chunks),
        out_shape=pltpu.VMEM((n_tok, feats), BF16),
        in_specs=[any_spec] * 6,
        out_specs=pl.BlockSpec(memory_space=pltpu.VMEM),
        scratch_shapes=[
            pltpu.VMEM((n_tok, n_z * fc), BF16),
            pltpu.VMEM((n_exp, group), jnp.int32),
            pltpu.VMEM((n_exp, group), F32),
            pltpu.VMEM((width, 2 * hidden), BF16),
            pltpu.VMEM((hidden, width), BF16),
            pltpu.VMEM((slots, n_tok), F32),
            pltpu.VMEM((n_tok, slots), BF16),
            pltpu.VMEM((n_tok, slots), BF16),
            pltpu.VMEM((slots, live), BF16),
            pltpu.VMEM((live, slots), BF16),
            pltpu.VMEM((n_exp, 1, 128), F32),
            pltpu.VMEM((n_ep, 1, 128), F32),
            pltpu.VMEM((n_z, slots, fc), BF16),
            pltpu.VMEM((n_z, slots, fc), BF16),
            pltpu.VMEM((chunks * n_tp, live, fc), BF16),
            pltpu.VMEM((live, 2 * hidden), F32),
            pltpu.VMEM((live, hidden), BF16),
            pltpu.VMEM((chunks * n_tp, live, fc), BF16),
            pltpu.VMEM((chunks * n_tp, live, fc), BF16),
            pltpu.VMEM((n_ret, slots, fc), BF16),
            pltpu.VMEM((n_ret, slots, fc), BF16),
            pltpu.VMEM((n_side, n_tok, fc), BF16),
            pltpu.VMEM((n_side, n_tok, fc), BF16),
        ],
        compiler_params=pltpu.CompilerParams(collective_id=0, has_side_effects=True),
    )(tokens, selected, affinity, w_gate, w_up, w_down)


def solution(mesh):
    placed = (
        P("ep", None),
        P(None, "ep"),
        P(None, "ep"),
        P("ep", None, "tp"),
        P("ep", None, "tp"),
        P("ep", "tp", None),
    )
    return jax.shard_map(
        per_device, mesh=mesh, in_specs=placed, out_specs=P("ep", "tp"), check_vma=False
    )
```

```python
import functools
import math

import jax
import jax.numpy as jnp
from jax import lax
from jax.experimental import pallas as pl
from jax.experimental.pallas import tpu as pltpu
from jax.sharding import PartitionSpec as P

MESH = pl.DeviceIdType.MESH
F32 = jnp.float32
BF16 = jnp.bfloat16
CHUNK = 128
OUT_EXTRA = 2
BACK = (0, 1)
SIDE_AT = 2


def side_of(n):
    s = math.isqrt(n)
    while n % s:
        s -= 1
    return s


def plan(n_tp, chunks):
    width = side_of(n_tp)
    height = n_tp // width
    offsets = [(dy, dx) for dy in range(height) for dx in range(width)][1:]
    far = sorted(offsets, key=lambda o: -((o[0] > 0) + (o[1] > 0)))
    square = (height, width) == (2, 2)
    extra = list(range(chunks))[max(0, chunks - OUT_EXTRA):] if square and chunks > OUT_EXTRA else []
    back = [c for c in BACK if square and chunks > max(BACK)]
    shared = [[o for o in far if not (c in extra and o == (1, 1))] for c in range(chunks)]
    reduced = [[o for o in far if not (c in back and o == (1, 1))] for c in range(chunks)]
    return width, height, far, extra, back, shared, reduced


def pieces_of(far, back, reduced, chunks):
    order = []
    for c in range(chunks):
        order += [(c, o) for o in reduced[c]]
        if c == 0:
            order += [(b, (1, 1)) for b in back]
    return order + [(c, (0, 0)) for c in range(chunks)]


def run(
    n_ep, n_tp, chunks,
    tok_hbm, sel_hbm, aff_hbm, wg_hbm, wu_hbm, wd_hbm, out_ref,
    tok, sel, aff, wgu, wd, onehot, weight_hi, weight_lo, expand, compact,
    cnt_out, cnt_in, z_out, z_in, rows, acc, hid, part_out, part_in, ret_out, ret_in,
    side_out, side_in,
    s_in, s_cnt, s_z_r, s_x_r, s_p_r, s_r_r, s_side_r, s_out,
):
    ep = lax.axis_index("ep")
    tp = lax.axis_index("tp")
    n_tok = tok.shape[0]
    n_exp, group = sel.shape
    fc = z_in.shape[2]
    feats = fc * chunks
    live = rows.shape[1]
    hidden = hid.shape[1]
    width, height, far, extra, back, shared, reduced = plan(n_tp, chunks)
    y, x = tp // width, lax.rem(tp, width)

    def tp_to(o):
        return lax.rem(y + o[0], height) * width + lax.rem(x + o[1], width)

    def tp_from(o):
        return lax.rem(y + height - o[0], height) * width + lax.rem(x + width - o[1], width)

    ep_order = list(range(n_ep - 1))
    high_half = ep // (n_ep // 2)

    def ep_to(i):
        down = n_ep - 1 - i
        down = down - jnp.where(down <= ep, 1, 0)
        up = i + jnp.where(i >= ep, 1, 0)
        return jnp.where(high_half > 0, up, down)

    def rows_of(i):
        return pl.ds(pl.multiple_of(i * group, group), group)

    def cols(k, c):
        return pl.ds(pl.multiple_of(k * feats + c * fc, 128), fc)

    def at(c, k):
        return c * n_tp + k

    z_chunks = [(c, (0, 0)) for c in range(chunks)] + [(c, (1, 1)) for c in extra]

    load_sel = pltpu.make_async_copy(sel_hbm, sel, s_in.at[0])
    load_sel.start()
    pltpu.make_async_copy(
        tok_hbm.at[:, pl.ds(pl.multiple_of(tp * feats, 128), feats)],
        tok.at[:, pl.ds(0, feats)], s_in.at[1]).start()
    if extra:
        first = extra[0] * fc
        start = pl.multiple_of(tp_to((1, 1)) * feats + first, 128)
        pltpu.make_async_copy(
            tok_hbm.at[:, pl.ds(start, feats - first)],
            tok.at[:, pl.ds(feats, feats - first)], s_in.at[1]).start()
    load_tok = pltpu.make_async_copy(tok, tok, s_in.at[1])

    barrier = pltpu.get_barrier_semaphore()
    for d in ep_order:
        pl.semaphore_signal(barrier, inc=1, device_id={"ep": ep_to(d)}, device_id_type=MESH)
    for o in far:
        pl.semaphore_signal(barrier, inc=1, device_id={"tp": tp_to(o)}, device_id_type=MESH)

    load_aff = pltpu.make_async_copy(aff_hbm, aff, s_in.at[2])
    load_aff.start()

    load_sel.wait()
    picked = sel[...].astype(F32)
    count = jnp.sum(jnp.where(picked >= 0, 1.0, 0.0), axis=1, keepdims=True)
    for e in range(n_exp):
        cnt_out[e] = jnp.broadcast_to(count[e:e + 1, :], (1, 128))
    picked_t = jnp.transpose(picked)
    token_lane = lax.broadcasted_iota(jnp.int32, (group, n_tok), 1).astype(F32)
    for e in range(n_exp):
        onehot[pl.ds(e * group, group), :] = jnp.where(
            picked_t[:, e:e + 1] == token_lane, 1.0, 0.0)
    load_tok.wait()
    pick = onehot[...].astype(BF16)

    def gather(i):
        z_out[i] = jnp.dot(
            pick, tok[:, i * fc:(i + 1) * fc], preferred_element_type=F32).astype(BF16)
        z_in[i, rows_of(ep), :] = z_out[i, rows_of(ep), :]

    gather(0)
    cnt_in[ep] = cnt_out[ep]

    pl.semaphore_wait(barrier, len(ep_order) + len(far))

    def send(src, dst, ss, rs, to):
        copy = pltpu.make_async_remote_copy(
            src_ref=src, dst_ref=dst, send_sem=ss, recv_sem=rs,
            device_id=to, device_id_type=MESH)
        copy.start()
        return copy

    others = (n_ep - 1) * group

    def whole(ref, ss, rs):
        return pltpu.make_async_remote_copy(
            src_ref=ref, dst_ref=ref, send_sem=ss, recv_sem=rs,
            device_id={"ep": ep_to(0)}, device_id_type=MESH)

    cnt_all = whole(cnt_in.at[pl.ds(0, n_ep - 1)], s_cnt.at[0], s_cnt.at[1])

    for d in ep_order:
        send(cnt_out.at[ep_to(d)], cnt_in.at[ep], s_cnt.at[0], s_cnt.at[1], {"ep": ep_to(d)})
    def spread_out(i):
        for d in ep_order:
            send(
                z_out.at[i, rows_of(ep_to(d)), :], z_in.at[i, rows_of(ep), :],
                s_out.at[0], s_z_r.at[i], {"ep": ep_to(d)})

    spread_out(0)
    first = min(3, chunks)
    for i in range(1, chunks):
        gather(i)
        if i < first:
            spread_out(i)

    pltpu.make_async_copy(wg_hbm.at[0], wgu.at[:, pl.ds(0, hidden)], s_in.at[3]).start()
    pltpu.make_async_copy(wu_hbm.at[0], wgu.at[:, pl.ds(hidden, hidden)], s_in.at[3]).start()
    load_w = pltpu.make_async_copy(wgu, wgu, s_in.at[3])
    for i in range(chunks, len(z_chunks)):
        gather(i)
    for i, (c, o) in enumerate(pieces_of(far, back, reduced, chunks)):
        pltpu.make_async_copy(
            wd_hbm.at[0, :, cols(tp_to(o), c)], wd.at[:, pl.ds(i * fc, fc)], s_in.at[4]).start()
    load_d = pltpu.make_async_copy(wd, wd, s_in.at[4])

    load_aff.wait()
    aff_t = jnp.transpose(aff[...])
    for e in range(n_exp):
        block = pl.ds(e * group, group)
        onehot[block, :] = onehot[block, :] * aff_t[:, e:e + 1]
    weight = jnp.transpose(onehot[...])
    high = weight.astype(BF16)
    weight_hi[...] = high
    weight_lo[...] = (weight - high.astype(F32)).astype(BF16)

    load_w.wait()
    acc[...] = jnp.zeros_like(acc)

    cnt_all.wait_recv()
    lane = lax.broadcasted_iota(jnp.int32, (group, live), 1).astype(F32)
    row = lax.broadcasted_iota(jnp.int32, (group, live), 0).astype(F32)
    begin = jnp.zeros((group, live), F32)
    pieces = []
    for j in range(n_ep):
        n = jnp.broadcast_to(cnt_in[j, 0:1, 0:1], (group, live))
        pieces.append(jnp.where((lane - row == begin) & (row < n), 1.0, 0.0))
        begin = begin + n
    spread = jnp.concatenate(pieces, axis=0)
    expand[...] = spread.astype(BF16)
    compact[...] = jnp.transpose(spread).astype(BF16)

    def take(c, k):
        acc[...] += jnp.dot(rows[at(c, k)], wgu[cols(k, c), :], preferred_element_type=F32)

    def squeeze(i):
        c, o = z_chunks[i]
        whole(z_in.at[i, pl.ds(0, others), :], s_out.at[0], s_z_r.at[i]).wait_recv()
        rows[at(c, tp_to(o))] = jnp.dot(
            compact[...], z_in[i], preferred_element_type=F32).astype(BF16)

    def arrive(c):
        whole(rows.at[pl.ds(0, len(shared[c]))], s_out.at[1], s_x_r.at[c]).wait_recv()

    for c in range(chunks):
        squeeze(c)
        for o in shared[c]:
            send(
                rows.at[at(c, tp)], rows.at[at(c, tp)],
                s_out.at[1], s_x_r.at[c], {"tp": tp_to(o)})
        if c == 0:
            for i in range(first, chunks):
                spread_out(i)
        if c == 1:
            for i in range(len(extra)):
                spread_out(chunks + i)
        take(c, tp)
    for c in range(chunks):
        if c in extra:
            squeeze(chunks + extra.index(c))
            take(c, tp_to((1, 1)))
        arrive(c)
        for o in shared[c]:
            take(c, tp_from(o))

    gate = acc[:, :hidden]
    up = acc[:, hidden:]
    hid[...] = (gate / (1.0 + jnp.exp(-gate)) * up).astype(BF16)
    load_d.wait()

    def give(i, value):
        ret_out[i] = jnp.dot(expand[...], value, preferred_element_type=F32).astype(BF16)
        for d in ep_order:
            send(
                ret_out.at[i, rows_of(ep_to(d)), :], ret_in.at[i, rows_of(ep), :],
                s_out.at[3], s_r_r.at[i], {"ep": ep_to(d)})
        ret_in[i, rows_of(ep), :] = ret_out[i, rows_of(ep), :]

    def combined(i):
        whole(ret_in.at[i, pl.ds(0, others), :], s_out.at[3], s_r_r.at[i]).wait_recv()
        value = ret_in[i]
        return (
            jnp.dot(weight_hi[...], value, preferred_element_type=F32)
            + jnp.dot(weight_lo[...], value, preferred_element_type=F32))

    order = pieces_of(far, back, reduced, chunks)
    step = max(1, 256 // fc)
    for i in range(0, len(order), step):
        some = order[i:i + step]
        value = jnp.dot(
            hid[...], wd[:, i * fc:(i + len(some)) * fc], preferred_element_type=F32).astype(BF16)
        for m, (c, o) in enumerate(some):
            k = tp_to(o)
            piece = value[:, m * fc:(m + 1) * fc]
            if o in reduced[c]:
                part_out[at(c, k)] = piece
                send(
                    part_out.at[at(c, k)], part_in.at[at(c, tp)],
                    s_out.at[2], s_p_r.at[c], {"tp": k})
            elif o == (0, 0):
                part_out[at(c, tp)] = piece
            else:
                give(chunks + back.index(c), piece)

    for c in range(chunks):
        total = part_out[at(c, tp)].astype(F32)
        whole(part_in.at[pl.ds(0, len(reduced[c]))], s_out.at[2], s_p_r.at[c]).wait_recv()
        for o in reduced[c]:
            total = total + part_in[at(c, tp_from(o))].astype(F32)
        give(c, total.astype(BF16))
        if c == min(SIDE_AT, chunks - 1):
            for b in range(len(back)):
                side_out[b] = combined(chunks + b).astype(BF16)
                send(
                    side_out.at[b], side_in.at[b],
                    s_out.at[4], s_side_r.at[b], {"tp": tp_to((1, 1))})

    cnt_all.wait_send()
    whole(z_in.at[:, pl.ds(0, others), :], s_out.at[0], s_z_r.at[0]).wait_send()
    n_x = sum(len(offsets) for offsets in shared)
    whole(rows.at[pl.ds(0, n_x)], s_out.at[1], s_x_r.at[0]).wait_send()
    n_p = sum(len(offsets) for offsets in reduced)
    whole(part_in.at[pl.ds(0, n_p)], s_out.at[2], s_p_r.at[0]).wait_send()

    for c in [1, 0, *range(2, chunks)] if back else range(chunks):
        value = combined(c)
        if c in back:
            b = back.index(c)
            whole(side_in.at[b], s_out.at[4], s_side_r.at[b]).wait_recv()
            value = value + side_in[b].astype(F32)
        out_ref[:, c * fc:(c + 1) * fc] = value.astype(BF16)

    if back:
        whole(side_in, s_out.at[4], s_side_r.at[0]).wait_send()
    whole(ret_in.at[:, pl.ds(0, others), :], s_out.at[3], s_r_r.at[0]).wait_send()


def kernel(n_ep, n_tp, chunks, *refs):
    n_z = chunks + len(plan(n_tp, chunks)[3])
    n_back = len(plan(n_tp, chunks)[4])
    dma = pltpu.SemaphoreType.DMA
    pl.run_scoped(
        functools.partial(run, n_ep, n_tp, chunks, *refs),
        dma((5,)), dma((2,)), dma((n_z,)), dma((chunks,)), dma((chunks,)), dma((chunks + n_back,)),
        dma((max(1, n_back),)), dma((5,)))


def per_device(tokens, selected, affinity, w_gate, w_up, w_down):
    n_ep = lax.axis_size("ep")
    n_tp = lax.axis_size("tp")
    n_tok, width = tokens.shape
    n_exp, group = selected.shape
    hidden = w_gate.shape[2]
    assert w_gate.shape[0] == 1 and n_exp == n_ep
    feats = width // n_tp
    chunks = max(1, feats // CHUNK)
    fc = feats // chunks
    n_z = chunks + len(plan(n_tp, chunks)[3])
    n_back = len(plan(n_tp, chunks)[4])
    n_ret = chunks + n_back
    n_side = max(1, n_back)
    slots = n_ep * group
    live = slots // 2
    any_spec = pl.BlockSpec(memory_space=pl.ANY)
    return pl.pallas_call(
        functools.partial(kernel, n_ep, n_tp, chunks),
        out_shape=pltpu.VMEM((n_tok, feats), BF16),
        in_specs=[any_spec] * 6,
        out_specs=pl.BlockSpec(memory_space=pltpu.VMEM),
        scratch_shapes=[
            pltpu.VMEM((n_tok, n_z * fc), BF16),
            pltpu.VMEM((n_exp, group), jnp.int32),
            pltpu.VMEM((n_exp, group), F32),
            pltpu.VMEM((width, 2 * hidden), BF16),
            pltpu.VMEM((hidden, width), BF16),
            pltpu.VMEM((slots, n_tok), F32),
            pltpu.VMEM((n_tok, slots), BF16),
            pltpu.VMEM((n_tok, slots), BF16),
            pltpu.VMEM((slots, live), BF16),
            pltpu.VMEM((live, slots), BF16),
            pltpu.VMEM((n_exp, 1, 128), F32),
            pltpu.VMEM((n_ep, 1, 128), F32),
            pltpu.VMEM((n_z, slots, fc), BF16),
            pltpu.VMEM((n_z, slots, fc), BF16),
            pltpu.VMEM((chunks * n_tp, live, fc), BF16),
            pltpu.VMEM((live, 2 * hidden), F32),
            pltpu.VMEM((live, hidden), BF16),
            pltpu.VMEM((chunks * n_tp, live, fc), BF16),
            pltpu.VMEM((chunks * n_tp, live, fc), BF16),
            pltpu.VMEM((n_ret, slots, fc), BF16),
            pltpu.VMEM((n_ret, slots, fc), BF16),
            pltpu.VMEM((n_side, n_tok, fc), BF16),
            pltpu.VMEM((n_side, n_tok, fc), BF16),
        ],
        compiler_params=pltpu.CompilerParams(collective_id=0, has_side_effects=True),
    )(tokens, selected, affinity, w_gate, w_up, w_down)


def solution(mesh):
    placed = (
        P("ep", None),
        P(None, "ep"),
        P(None, "ep"),
        P("ep", None, "tp"),
        P("ep", None, "tp"),
        P("ep", "tp", None),
    )
    return jax.shard_map(
        per_device, mesh=mesh, in_specs=placed, out_specs=P("ep", "tp"), check_vma=False
    )
```

```python
import functools
import math

import jax
import jax.numpy as jnp
from jax import lax
from jax.experimental import pallas as pl
from jax.experimental.pallas import tpu as pltpu
from jax.sharding import PartitionSpec as P

MESH = pl.DeviceIdType.MESH
F32 = jnp.float32
BF16 = jnp.bfloat16
CHUNK = 128
OUT_EXTRA = 2
BACK = (0, 1)
SIDE_AT = 2


def side_of(n):
    s = math.isqrt(n)
    while n % s:
        s -= 1
    return s


def plan(n_tp, chunks):
    width = side_of(n_tp)
    height = n_tp // width
    offsets = [(dy, dx) for dy in range(height) for dx in range(width)][1:]
    far = sorted(offsets, key=lambda o: -((o[0] > 0) + (o[1] > 0)))
    square = (height, width) == (2, 2)
    extra = list(range(chunks))[max(0, chunks - OUT_EXTRA):] if square and chunks > OUT_EXTRA else []
    back = [c for c in BACK if square and chunks > max(BACK)]
    shared = [[o for o in far if not (c in extra and o == (1, 1))] for c in range(chunks)]
    reduced = [[o for o in far if not (c in back and o == (1, 1))] for c in range(chunks)]
    return width, height, far, extra, back, shared, reduced


def pieces_of(far, back, reduced, chunks):
    order = []
    for c in range(chunks):
        order += [(c, (1, 1))] * (c in back) + [(c, o) for o in reduced[c]]
    return order + [(c, (0, 0)) for c in range(chunks)]


def run(
    n_ep, n_tp, chunks,
    tok_hbm, sel_hbm, aff_hbm, wg_hbm, wu_hbm, wd_hbm, out_ref,
    tok, sel, aff, wgu, wd, onehot, weight_hi, weight_lo, expand, compact,
    cnt_out, cnt_in, z_out, z_in, rows, acc, hid, part_out, part_in, ret_out, ret_in,
    side_out, side_in,
    s_in, s_cnt, s_z_r, s_x_r, s_p_r, s_r_r, s_side_r, s_out,
):
    ep = lax.axis_index("ep")
    tp = lax.axis_index("tp")
    n_tok = tok.shape[0]
    n_exp, group = sel.shape
    fc = z_in.shape[2]
    feats = fc * chunks
    live = rows.shape[1]
    hidden = hid.shape[1]
    width, height, far, extra, back, shared, reduced = plan(n_tp, chunks)
    y, x = tp // width, lax.rem(tp, width)

    def tp_to(o):
        return lax.rem(y + o[0], height) * width + lax.rem(x + o[1], width)

    def tp_from(o):
        return lax.rem(y + height - o[0], height) * width + lax.rem(x + width - o[1], width)

    ep_order = list(range(n_ep - 1))
    high_half = ep // (n_ep // 2)

    def ep_to(i):
        down = n_ep - 1 - i
        down = down - jnp.where(down <= ep, 1, 0)
        up = i + jnp.where(i >= ep, 1, 0)
        return jnp.where(high_half > 0, up, down)

    def rows_of(i):
        return pl.ds(pl.multiple_of(i * group, group), group)

    def cols(k, c):
        return pl.ds(pl.multiple_of(k * feats + c * fc, 128), fc)

    def at(c, k):
        return c * n_tp + k

    z_chunks = [(c, (0, 0)) for c in range(chunks)] + [(c, (1, 1)) for c in extra]

    load_sel = pltpu.make_async_copy(sel_hbm, sel, s_in.at[0])
    load_sel.start()
    pltpu.make_async_copy(
        tok_hbm.at[:, pl.ds(pl.multiple_of(tp * feats, 128), feats)],
        tok.at[:, pl.ds(0, feats)], s_in.at[1]).start()
    if extra:
        first = extra[0] * fc
        start = pl.multiple_of(tp_to((1, 1)) * feats + first, 128)
        pltpu.make_async_copy(
            tok_hbm.at[:, pl.ds(start, feats - first)],
            tok.at[:, pl.ds(feats, feats - first)], s_in.at[1]).start()
    load_tok = pltpu.make_async_copy(tok, tok, s_in.at[1])

    barrier = pltpu.get_barrier_semaphore()
    for d in ep_order:
        pl.semaphore_signal(barrier, inc=1, device_id={"ep": ep_to(d)}, device_id_type=MESH)
    for o in far:
        pl.semaphore_signal(barrier, inc=1, device_id={"tp": tp_to(o)}, device_id_type=MESH)

    load_aff = pltpu.make_async_copy(aff_hbm, aff, s_in.at[2])
    load_aff.start()

    load_sel.wait()
    picked = sel[...].astype(F32)
    count = jnp.sum(jnp.where(picked >= 0, 1.0, 0.0), axis=1, keepdims=True)
    for e in range(n_exp):
        cnt_out[e] = jnp.broadcast_to(count[e:e + 1, :], (1, 128))
    picked_t = jnp.transpose(picked)
    token_lane = lax.broadcasted_iota(jnp.int32, (group, n_tok), 1).astype(F32)
    for e in range(n_exp):
        onehot[pl.ds(e * group, group), :] = jnp.where(
            picked_t[:, e:e + 1] == token_lane, 1.0, 0.0)
    load_tok.wait()
    pick = onehot[...].astype(BF16)

    def gather(i):
        z_out[i] = jnp.dot(
            pick, tok[:, i * fc:(i + 1) * fc], preferred_element_type=F32).astype(BF16)
        z_in[i, rows_of(ep), :] = z_out[i, rows_of(ep), :]

    gather(0)
    cnt_in[ep] = cnt_out[ep]

    pl.semaphore_wait(barrier, len(ep_order) + len(far))

    def send(src, dst, ss, rs, to):
        copy = pltpu.make_async_remote_copy(
            src_ref=src, dst_ref=dst, send_sem=ss, recv_sem=rs,
            device_id=to, device_id_type=MESH)
        copy.start()
        return copy

    others = (n_ep - 1) * group

    def whole(ref, ss, rs):
        return pltpu.make_async_remote_copy(
            src_ref=ref, dst_ref=ref, send_sem=ss, recv_sem=rs,
            device_id={"ep": ep_to(0)}, device_id_type=MESH)

    cnt_all = whole(cnt_in.at[pl.ds(0, n_ep - 1)], s_cnt.at[0], s_cnt.at[1])

    for d in ep_order:
        send(cnt_out.at[ep_to(d)], cnt_in.at[ep], s_cnt.at[0], s_cnt.at[1], {"ep": ep_to(d)})
    def spread_out(i):
        for d in ep_order:
            send(
                z_out.at[i, rows_of(ep_to(d)), :], z_in.at[i, rows_of(ep), :],
                s_out.at[0], s_z_r.at[i], {"ep": ep_to(d)})

    spread_out(0)
    first = min(3, chunks)
    for i in range(1, chunks):
        gather(i)
        if i < first:
            spread_out(i)

    pltpu.make_async_copy(wg_hbm.at[0], wgu.at[:, pl.ds(0, hidden)], s_in.at[3]).start()
    pltpu.make_async_copy(wu_hbm.at[0], wgu.at[:, pl.ds(hidden, hidden)], s_in.at[3]).start()
    load_w = pltpu.make_async_copy(wgu, wgu, s_in.at[3])
    for i in range(chunks, len(z_chunks)):
        gather(i)
    for i, (c, o) in enumerate(pieces_of(far, back, reduced, chunks)):
        pltpu.make_async_copy(
            wd_hbm.at[0, :, cols(tp_to(o), c)], wd.at[:, pl.ds(i * fc, fc)], s_in.at[4]).start()
    load_d = pltpu.make_async_copy(wd, wd, s_in.at[4])

    load_aff.wait()
    aff_t = jnp.transpose(aff[...])
    for e in range(n_exp):
        block = pl.ds(e * group, group)
        onehot[block, :] = onehot[block, :] * aff_t[:, e:e + 1]
    weight = jnp.transpose(onehot[...])
    high = weight.astype(BF16)
    weight_hi[...] = high
    weight_lo[...] = (weight - high.astype(F32)).astype(BF16)

    load_w.wait()
    acc[...] = jnp.zeros_like(acc)

    cnt_all.wait_recv()
    lane = lax.broadcasted_iota(jnp.int32, (group, live), 1).astype(F32)
    row = lax.broadcasted_iota(jnp.int32, (group, live), 0).astype(F32)
    begin = jnp.zeros((group, live), F32)
    pieces = []
    for j in range(n_ep):
        n = jnp.broadcast_to(cnt_in[j, 0:1, 0:1], (group, live))
        pieces.append(jnp.where((lane - row == begin) & (row < n), 1.0, 0.0))
        begin = begin + n
    spread = jnp.concatenate(pieces, axis=0)
    expand[...] = spread.astype(BF16)
    compact[...] = jnp.transpose(spread).astype(BF16)

    def take(c, k):
        acc[...] += jnp.dot(rows[at(c, k)], wgu[cols(k, c), :], preferred_element_type=F32)

    def squeeze(i):
        c, o = z_chunks[i]
        whole(z_in.at[i, pl.ds(0, others), :], s_out.at[0], s_z_r.at[i]).wait_recv()
        rows[at(c, tp_to(o))] = jnp.dot(
            compact[...], z_in[i], preferred_element_type=F32).astype(BF16)

    def arrive(c):
        whole(rows.at[pl.ds(0, len(shared[c]))], s_out.at[1], s_x_r.at[c]).wait_recv()

    for c in range(chunks):
        squeeze(c)
        for o in shared[c]:
            send(
                rows.at[at(c, tp)], rows.at[at(c, tp)],
                s_out.at[1], s_x_r.at[c], {"tp": tp_to(o)})
        if c == 0:
            for i in range(first, chunks):
                spread_out(i)
        if c == 1:
            for i in range(len(extra)):
                spread_out(chunks + i)
        take(c, tp)
    for c in range(chunks):
        if c in extra:
            squeeze(chunks + extra.index(c))
            take(c, tp_to((1, 1)))
        arrive(c)
        for o in shared[c]:
            take(c, tp_from(o))

    gate = acc[:, :hidden]
    up = acc[:, hidden:]
    hid[...] = (gate / (1.0 + jnp.exp(-gate)) * up).astype(BF16)
    load_d.wait()

    def give(i, value):
        ret_out[i] = jnp.dot(expand[...], value, preferred_element_type=F32).astype(BF16)
        for d in ep_order:
            send(
                ret_out.at[i, rows_of(ep_to(d)), :], ret_in.at[i, rows_of(ep), :],
                s_out.at[3], s_r_r.at[i], {"ep": ep_to(d)})
        ret_in[i, rows_of(ep), :] = ret_out[i, rows_of(ep), :]

    def combined(i):
        whole(ret_in.at[i, pl.ds(0, others), :], s_out.at[3], s_r_r.at[i]).wait_recv()
        value = ret_in[i]
        return (
            jnp.dot(weight_hi[...], value, preferred_element_type=F32)
            + jnp.dot(weight_lo[...], value, preferred_element_type=F32))

    order = pieces_of(far, back, reduced, chunks)
    step = max(1, 256 // fc)
    for i in range(0, len(order), step):
        some = order[i:i + step]
        value = jnp.dot(
            hid[...], wd[:, i * fc:(i + len(some)) * fc], preferred_element_type=F32).astype(BF16)
        for m, (c, o) in enumerate(some):
            k = tp_to(o)
            piece = value[:, m * fc:(m + 1) * fc]
            if o in reduced[c]:
                part_out[at(c, k)] = piece
                send(
                    part_out.at[at(c, k)], part_in.at[at(c, tp)],
                    s_out.at[2], s_p_r.at[c], {"tp": k})
            elif o == (0, 0):
                part_out[at(c, tp)] = piece
            else:
                give(chunks + back.index(c), piece)

    for c in range(chunks):
        total = part_out[at(c, tp)].astype(F32)
        whole(part_in.at[pl.ds(0, len(reduced[c]))], s_out.at[2], s_p_r.at[c]).wait_recv()
        for o in reduced[c]:
            total = total + part_in[at(c, tp_from(o))].astype(F32)
        give(c, total.astype(BF16))
        if c == min(SIDE_AT, chunks - 1):
            for b in range(len(back)):
                side_out[b] = combined(chunks + b).astype(BF16)
                send(
                    side_out.at[b], side_in.at[b],
                    s_out.at[4], s_side_r.at[b], {"tp": tp_to((1, 1))})

    cnt_all.wait_send()
    whole(z_in.at[:, pl.ds(0, others), :], s_out.at[0], s_z_r.at[0]).wait_send()
    n_x = sum(len(offsets) for offsets in shared)
    whole(rows.at[pl.ds(0, n_x)], s_out.at[1], s_x_r.at[0]).wait_send()
    n_p = sum(len(offsets) for offsets in reduced)
    whole(part_in.at[pl.ds(0, n_p)], s_out.at[2], s_p_r.at[0]).wait_send()

    for c in [1, 0, *range(2, chunks)] if back else range(chunks):
        value = combined(c)
        if c in back:
            b = back.index(c)
            whole(side_in.at[b], s_out.at[4], s_side_r.at[b]).wait_recv()
            value = value + side_in[b].astype(F32)
        out_ref[:, c * fc:(c + 1) * fc] = value.astype(BF16)

    if back:
        whole(side_in, s_out.at[4], s_side_r.at[0]).wait_send()
    whole(ret_in.at[:, pl.ds(0, others), :], s_out.at[3], s_r_r.at[0]).wait_send()


def kernel(n_ep, n_tp, chunks, *refs):
    n_z = chunks + len(plan(n_tp, chunks)[3])
    n_back = len(plan(n_tp, chunks)[4])
    dma = pltpu.SemaphoreType.DMA
    pl.run_scoped(
        functools.partial(run, n_ep, n_tp, chunks, *refs),
        dma((5,)), dma((2,)), dma((n_z,)), dma((chunks,)), dma((chunks,)), dma((chunks + n_back,)),
        dma((max(1, n_back),)), dma((5,)))


def per_device(tokens, selected, affinity, w_gate, w_up, w_down):
    n_ep = lax.axis_size("ep")
    n_tp = lax.axis_size("tp")
    n_tok, width = tokens.shape
    n_exp, group = selected.shape
    hidden = w_gate.shape[2]
    assert w_gate.shape[0] == 1 and n_exp == n_ep
    feats = width // n_tp
    chunks = max(1, feats // CHUNK)
    fc = feats // chunks
    n_z = chunks + len(plan(n_tp, chunks)[3])
    n_back = len(plan(n_tp, chunks)[4])
    n_ret = chunks + n_back
    n_side = max(1, n_back)
    slots = n_ep * group
    live = slots // 2
    any_spec = pl.BlockSpec(memory_space=pl.ANY)
    return pl.pallas_call(
        functools.partial(kernel, n_ep, n_tp, chunks),
        out_shape=pltpu.VMEM((n_tok, feats), BF16),
        in_specs=[any_spec] * 6,
        out_specs=pl.BlockSpec(memory_space=pltpu.VMEM),
        scratch_shapes=[
            pltpu.VMEM((n_tok, n_z * fc), BF16),
            pltpu.VMEM((n_exp, group), jnp.int32),
            pltpu.VMEM((n_exp, group), F32),
            pltpu.VMEM((width, 2 * hidden), BF16),
            pltpu.VMEM((hidden, width), BF16),
            pltpu.VMEM((slots, n_tok), F32),
            pltpu.VMEM((n_tok, slots), BF16),
            pltpu.VMEM((n_tok, slots), BF16),
            pltpu.VMEM((slots, live), BF16),
            pltpu.VMEM((live, slots), BF16),
            pltpu.VMEM((n_exp, 1, 128), F32),
            pltpu.VMEM((n_ep, 1, 128), F32),
            pltpu.VMEM((n_z, slots, fc), BF16),
            pltpu.VMEM((n_z, slots, fc), BF16),
            pltpu.VMEM((chunks * n_tp, live, fc), BF16),
            pltpu.VMEM((live, 2 * hidden), F32),
            pltpu.VMEM((live, hidden), BF16),
            pltpu.VMEM((chunks * n_tp, live, fc), BF16),
            pltpu.VMEM((chunks * n_tp, live, fc), BF16),
            pltpu.VMEM((n_ret, slots, fc), BF16),
            pltpu.VMEM((n_ret, slots, fc), BF16),
            pltpu.VMEM((n_side, n_tok, fc), BF16),
            pltpu.VMEM((n_side, n_tok, fc), BF16),
        ],
        compiler_params=pltpu.CompilerParams(collective_id=0, has_side_effects=True),
    )(tokens, selected, affinity, w_gate, w_up, w_down)


def solution(mesh):
    placed = (
        P("ep", None),
        P(None, "ep"),
        P(None, "ep"),
        P("ep", None, "tp"),
        P("ep", None, "tp"),
        P("ep", "tp", None),
    )
    return jax.shard_map(
        per_device, mesh=mesh, in_specs=placed, out_specs=P("ep", "tp"), check_vma=False
    )
```
